512 devices in a mesh: ep: 32 (over z, x), tp: 16 (over y, core).
Axes of the slice: x: 4, y: 8, z: 8, core: 2. Of those that a mesh axis runs over, the one named last changes fastest.
Arguments:
- queries: bfloat16 [16384, 2048], P('ep', 'tp'), may hold values from -6 to 6
- keys: bfloat16 [16384, 2048], P('ep', 'tp'), may hold values from -12 to 12
- values: bfloat16 [16384, 2048], P('ep', 'tp'), may hold values from -8 to 8
- key_bias: bfloat16 [16384, 16], P('ep', 'tp'), may hold values from -16 to 0
- out_weight: bfloat16 [2048, 2048], P('tp'), may hold values from -0.1875 to 0.1875
- moe_input: bfloat16 [4096, 2048], P('ep'), may hold values from -6 to 6
- moe_gain: float32 [2048], replicated, may hold values from 0.1 to 1.9
- route_ids: int32 [4096, 2], P('ep'), may hold values from 0 to 31, all different within a row; in each aligned block of 128 rows (0 to 127, 128 to 255, ...) at most 12 rows name the same one
- route_scores: float32 [4096, 2], P('ep'), may hold values from 0.05 to 1
- shared_gate: bfloat16 [2048, 2048], P(None, 'tp'), may hold values from -0.125 to 0.125
- shared_up: bfloat16 [2048, 2048], P(None, 'tp'), may hold values from -0.125 to 0.125
- shared_down: bfloat16 [2048, 2048], P('tp'), may hold values from -0.1875 to 0.1875
- expert_gate: bfloat16 [32, 2048, 2048], P('ep', None, 'tp'), may hold values from -0.125 to 0.125
- expert_up: bfloat16 [32, 2048, 2048], P('ep', None, 'tp'), may hold values from -0.125 to 0.125
- expert_down: bfloat16 [32, 2048, 2048], P('ep', 'tp'), may hold values from -0.1875 to 0.1875
Outputs:
- mixed_tokens: bfloat16 [16384, 2048], P('ep', 'tp')
- expert_mix: bfloat16 [4096, 2048], P('ep', 'tp')
The draws below stay inside these ranges and needn't reach their ends.
Inputs may be any that keep to these rules, and one draw needn't show every extreme that they name: `route_ids`: each row names 2 different experts. Among the 128 rows of one index of ep no expert is named by more than 12 rows, and in some such block one expert is named by exactly 12 rows.
All inputs are finite; a program needn't handle non-finite values.
Results may differ from the reference program's by a relative error of at most 0.019.
Values may be sent and summed in bfloat16 or wider, within the bound.
A program may use at most 128 MiB of HBM per device.

```python
import math
import jax
import jax.numpy as jnp
import numpy as np
from jax import lax

D = 2048
HEADS = 16
HD = 128
F = 2048
FSH = 2048
TOPK = 2
SEQUENCE_COUNT = 1
ROWS_A = 512
ROWS_M = 128
ATTENTION_TOKENS = 16384
SEQUENCE_LENGTH = 16384
TOKENS_M = 4096
EXPERTS = 32
CAP = 12
N_EP = 32
N_TP = 16


def draw_key_bias(key, part):
    draw_keys = jax.random.split(key, 7)
    fast_share = 0.5
    fast_head = jax.random.uniform(draw_keys[0], (HEADS,)) < fast_share
    fast_rate = jnp.exp(jax.random.uniform(draw_keys[1], (HEADS,), minval=jnp.log(1.0 / 100.0), maxval=jnp.log(1.0 / 30.0)))
    slow_rate = jnp.exp(jax.random.uniform(draw_keys[2], (HEADS,), minval=jnp.log(0.3 / SEQUENCE_LENGTH), maxval=jnp.log(1.2 / SEQUENCE_LENGTH)))
    base_logit = jnp.log(jnp.where(fast_head, fast_rate, slow_rate)) - 2.15
    block_count = ATTENTION_TOKENS // ROWS_A
    block_shift = jax.random.uniform(draw_keys[3], (block_count, 1, HEADS), minval=-0.7, maxval=0.7)
    jitter = jax.random.uniform(draw_keys[4], (block_count, ROWS_A, HEADS), minval=-0.7, maxval=0.7)
    smoothing_factor = (base_logit[None, None, :] + block_shift + jitter).reshape(ATTENTION_TOKENS, HEADS)
    spike_position = jax.random.randint(draw_keys[5], (SEQUENCE_COUNT, 2), 0, SEQUENCE_LENGTH)
    token_position = jnp.arange(ATTENTION_TOKENS) % SEQUENCE_LENGTH
    sequence_index = jnp.arange(ATTENTION_TOKENS) // SEQUENCE_LENGTH
    spike_mask = jnp.any(token_position[:, None] == spike_position[sequence_index], axis=1)
    spike_fraction = jax.random.uniform(draw_keys[6], (ATTENTION_TOKENS, 1), minval=0.2, maxval=0.4)
    spike_logit = jnp.log(spike_fraction) - jnp.log(1.0 - spike_fraction)
    return jnp.where(spike_mask[:, None], spike_logit, smoothing_factor).astype(jnp.float32).astype(jnp.bfloat16)


def draw_values(key, part):
    draw_keys = jax.random.split(key, 3)
    block_count = ATTENTION_TOKENS // ROWS_A
    sign = jnp.where(jax.random.uniform(draw_keys[0], (HEADS,)) < 0.5, -1.0, 1.0)
    size = jax.random.uniform(draw_keys[1], (block_count, 1, HEADS, 1), minval=0.5, maxval=1.5)
    noise = jnp.clip(1.5 * jax.random.normal(draw_keys[2], (block_count, ROWS_A, HEADS, HD)), -6.0, 6.0)
    mixed = sign[None, None, :, None] * size + noise
    return mixed.reshape(ATTENTION_TOKENS, HEADS * HD).astype(jnp.float32).astype(jnp.bfloat16)


def with_spikes(array, rng, source, target, blocks, factor):
    def block_of(axis_at):
        return (jnp.arange(array.shape[axis_at]) // (array.shape[axis_at] // blocks)).reshape((-1,) + (1,) * (array.ndim - 1 - axis_at))

    one_side = jax.random.permutation(rng, blocks)[block_of(target)]
    far = (block_of(target) + blocks // 2) % blocks
    return jnp.where((block_of(source) == one_side) | (block_of(source) == far), factor * array, array)


def level_of(rng, extent, cuts, low, top_value):
    gain = 1.0
    for position, shards_of in cuts:
        heights = jax.random.uniform(jax.random.fold_in(jax.random.fold_in(rng, 6), position), (shards_of,), jnp.float32, low / len(cuts), top_value / len(cuts))
        gain = gain * jnp.repeat(jnp.exp(heights), extent[position] // shards_of).reshape((-1,) + (1,) * (len(extent) - 1 - position))
    return gain


def routed_block(key, own, number, rows, count, top, most, slope):
    order = jax.random.permutation(key, count)
    crowded, usual = portions_of(count, rows * top, most, slope, True), portions_of(count, rows * top, most, slope, False)
    places = jnp.arange(count)

    def named(lengths, offset_by):
        used = int((lengths > 0).sum())
        fixed = max(1, used // 4)
        shifted = fixed + (places - fixed + offset_by * (used - fixed)) % max(1, count - fixed)
        return jnp.zeros((count,), jnp.int32).at[order[jnp.where(places < fixed, places, shifted)]].set(jnp.asarray(lengths, jnp.int32))

    lengths = jnp.where(number % 4 == 0, named(crowded, number // 4), named(usual, number - number // 4 - 1))
    mixed = jax.random.permutation(jax.random.fold_in(own, 3), count)
    donor, sink = mixed[0:count // 2 * 2:2], mixed[1:count // 2 * 2:2]
    slack = jnp.minimum(lengths[donor] - 1, most - lengths[sink]) // 2
    slack = jnp.where((donor == order[0]) | (sink == order[0]) | (lengths[sink] == 0), 0, jnp.maximum(slack, 0))
    shifted = jax.random.randint(jax.random.fold_in(own, 4), (count // 2,), 0, 1 << 20) % (slack + 1)
    lengths = lengths.at[donor].add(-shifted).at[sink].add(shifted)
    members = jnp.searchsorted(jnp.cumsum(lengths), jnp.arange(rows * top), side="right").astype(jnp.int32)
    table = members.reshape(top, rows).T
    table = table[jax.random.permutation(jax.random.fold_in(own, 1), rows)]
    offset_by = jax.random.randint(jax.random.fold_in(own, 2), (rows, 1), 0, top)
    return jnp.take_along_axis(table, (jnp.arange(top)[None, :] + offset_by) % top, axis=1)


def portions_of(count, total, limit, lean, full):
    portions = [(1 << 20) // math.isqrt(standing ** lean) + 1 for standing in range(1, count + 1)]
    largest = limit if full else min(limit, max(-(-total // count), total * portions[0] // sum(portions)))
    least = 1 if total - largest >= count - 1 else 0
    holding, surplus = [largest] + [least] * (count - 1), total - largest - least * (count - 1)
    while surplus > 0:
        free = [i for i in range(1, count) if holding[i] < largest] or [i for i in range(1, count) if holding[i] < limit]
        mass, left = sum([portions[i] for i in free]), surplus
        for i in free:
            extra = min(limit - holding[i], max(1, left * portions[i] // mass), surplus)
            holding[i] = holding[i] + extra
            surplus = surplus - extra
    return np.array(holding)


def centred(rng, extent, deviation, most, shards=(), kind=jnp.bfloat16):
    gain = level_of(rng, extent, shards, -0.22, 0.18) if shards else 1.0
    values = jax.random.normal(rng, extent, jnp.float32) * deviation * gain
    return jnp.minimum(jnp.maximum(values, -most), most).astype(kind)


def gaussian_with(stream_key, dims, scale, limit, shards, heavy, held_as=jnp.bfloat16):
    array = scale * jax.random.normal(stream_key, dims, jnp.float32)
    if shards:
        array = array * level_of(stream_key, dims, shards, -0.22, 0.18)
    return jnp.clip(with_spikes(array, jax.random.fold_in(stream_key, 3), *heavy), -limit, limit).astype(held_as)


def setup_inputs(seed: int = 0) -> dict:
    streams_of = jax.random.split(jax.random.key(seed), 16)
    queries = centred(streams_of[0], (ATTENTION_TOKENS, HEADS * HD), 1.0, 6.0, ((0, 32), (1, 16)))
    keys = centred(streams_of[1], (ATTENTION_TOKENS, HEADS * HD), 2.0, 12.0, ((0, 32), (1, 16)))
    values = draw_values(jax.random.fold_in(streams_of[15], 71), 0)
    key_bias = draw_key_bias(jax.random.fold_in(streams_of[15], 71), 0)
    out_weight = gaussian_with(streams_of[4], (HEADS * HD, D), (HEADS * HD) ** -0.5, 0.1875, ((0, 16),), (0, 1, 16, 2.0))
    moe_input = centred(streams_of[5], (TOKENS_M, D), 1.0, 6.0, ((0, 32),))
    moe_gain = jnp.clip(1.0 + 0.18 * jax.random.normal(streams_of[6], (D,), jnp.float32), 0.1, 1.9)
    route_ids_keys = jax.random.split(jax.random.fold_in(streams_of[7], 1), TOKENS_M // ROWS_M)
    route_ids_turns = jax.random.permutation(jax.random.fold_in(streams_of[7], 3), TOKENS_M // ROWS_M)
    route_ids = jax.vmap(lambda own, number: routed_block(jax.random.fold_in(streams_of[7], 2), own, number, ROWS_M, EXPERTS, TOPK, CAP, 2))(route_ids_keys, route_ids_turns).reshape((TOKENS_M, TOPK))
    route_scores = jnp.clip(0.05 + 0.95 * jax.random.uniform(streams_of[8], (TOKENS_M, TOPK), jnp.float32) ** level_of(streams_of[8], (TOKENS_M, TOPK), ((0, 32),), -0.2, 0.2), 0.05, 1.0)
    shared_gate = centred(streams_of[9], (D, FSH), D ** -0.5, 0.125, ((1, 16),))
    shared_up = centred(streams_of[10], (D, FSH), D ** -0.5, 0.125, ((1, 16),))
    shared_down = gaussian_with(streams_of[11], (FSH, D), FSH ** -0.5, 0.1875, ((0, 16),), (0, 1, 16, 2.0))
    expert_gate = centred(streams_of[12], (EXPERTS, D, F), D ** -0.5, 0.125, ((0, 32), (2, 16)))
    expert_up = centred(streams_of[13], (EXPERTS, D, F), D ** -0.5, 0.125, ((0, 32), (2, 16)))
    expert_down = gaussian_with(streams_of[14], (EXPERTS, F, D), F ** -0.5, 0.1875, ((0, 32), (1, 16)), (1, 2, 16, 2.0))
    return {"queries": queries, "keys": keys, "values": values, "key_bias": key_bias, "out_weight": out_weight, "moe_input": moe_input, "moe_gain": moe_gain, "route_ids": route_ids, "route_scores": route_scores, "shared_gate": shared_gate, "shared_up": shared_up, "shared_down": shared_down, "expert_gate": expert_gate, "expert_up": expert_up, "expert_down": expert_down}


EPS_NORM = 1e-06
ROUTED_SCALE = 2.5

def head_span(query_head, key_head, value_head, bias_head):
    length = query_head.shape[0]
    block = min(512, length)
    scale = HD ** (-0.5)
    key_pos = jnp.arange(length, dtype=jnp.int32)
    bias_row = bias_head.astype(jnp.float32)[None, :]

    def one_block(start):
        query_block = lax.dynamic_slice_in_dim(query_head, start, block, 0)
        logit = jnp.dot(query_block, key_head.T, preferred_element_type=jnp.float32) * scale + bias_row
        query_pos = start + jnp.arange(block, dtype=jnp.int32)
        visible = key_pos[None, :] < query_pos[:, None]
        keep = jnp.where(visible, jax.nn.log_sigmoid(-logit), 0.0)
        stay = lax.cumsum(keep, axis=1, reverse=True) - keep
        weight = jnp.where(visible, jnp.exp(jax.nn.log_sigmoid(logit) + stay), 0.0).astype(jnp.bfloat16)
        return jnp.dot(weight, value_head, preferred_element_type=jnp.float32).astype(jnp.bfloat16)
    starts = jnp.arange(length // block, dtype=jnp.int32) * block
    return lax.map(one_block, starts).reshape(length, -1)

def per_head(operands):
    return head_span(operands[0], operands[1], operands[2], operands[3])

def grouped_sum(left, right, groups):
    width = left.shape[1] // groups
    total = jnp.zeros((left.shape[0], right.shape[1]), jnp.float32)
    for group in range(groups):
        partial_sum = jnp.dot(left[:, group * width:(group + 1) * width], right[group * width:(group + 1) * width], preferred_element_type=jnp.float32)
        rounded = lax.optimization_barrier(partial_sum.astype(jnp.bfloat16))
        total = total + rounded.astype(jnp.float32)
    return total

def one_expert(operands):
    rows_in, weight_gate, weight_up, weight_down = operands
    gate_part = jnp.dot(rows_in, weight_gate, preferred_element_type=jnp.float32)
    up_part = jnp.dot(rows_in, weight_up, preferred_element_type=jnp.float32)
    hidden = (jax.nn.silu(gate_part) * up_part).astype(jnp.bfloat16)
    return grouped_sum(hidden, weight_down, N_TP).astype(jnp.bfloat16)

def reference(queries, keys, values, key_bias, out_weight, moe_input, moe_gain, route_ids, route_scores, shared_gate, shared_up, shared_down, expert_gate, expert_up, expert_down):
    pieces = []
    for sequence_index in range(SEQUENCE_COUNT):
        first = sequence_index * SEQUENCE_LENGTH
        query_seq = queries[first:first + SEQUENCE_LENGTH].reshape(SEQUENCE_LENGTH, HEADS, HD).transpose(1, 0, 2)
        key_seq = keys[first:first + SEQUENCE_LENGTH].reshape(SEQUENCE_LENGTH, HEADS, HD).transpose(1, 0, 2)
        value_seq = values[first:first + SEQUENCE_LENGTH].reshape(SEQUENCE_LENGTH, HEADS, HD).transpose(1, 0, 2)
        bias_seq = key_bias[first:first + SEQUENCE_LENGTH].T
        head_outs = lax.map(per_head, (query_seq, key_seq, value_seq, bias_seq))
        pieces.append(head_outs.transpose(1, 0, 2).reshape(SEQUENCE_LENGTH, HEADS * HD))
    heads_out = jnp.concatenate(pieces, axis=0)
    mixed_tokens = grouped_sum(heads_out, out_weight, N_TP).astype(jnp.bfloat16)
    inputs = moe_input.astype(jnp.float32)
    normed = (inputs * lax.rsqrt(lax.optimization_barrier(jnp.mean(inputs * inputs, axis=-1, keepdims=True)) + EPS_NORM) * moe_gain.astype(jnp.float32)).astype(jnp.bfloat16)
    shared_hidden = (jax.nn.silu(jnp.dot(normed, shared_gate, preferred_element_type=jnp.float32)) * jnp.dot(normed, shared_up, preferred_element_type=jnp.float32)).astype(jnp.bfloat16)
    shared_result = grouped_sum(shared_hidden, shared_down, N_TP)
    chosen = route_ids.reshape(N_EP, ROWS_M * TOPK).astype(jnp.int32)
    onehot = (chosen[:, :, None] == jnp.arange(EXPERTS, dtype=jnp.int32)[None, None, :]).astype(jnp.int32)
    place = lax.optimization_barrier(jnp.sum((jnp.cumsum(onehot, axis=1) - onehot) * onehot, axis=2))
    block_ids = jnp.arange(N_EP, dtype=jnp.int32)[:, None]
    slot_index = (chosen * (N_EP * CAP) + block_ids * CAP + place).reshape(-1).astype(jnp.int32)
    token_index = jnp.arange(TOKENS_M * TOPK, dtype=jnp.int32) // TOPK
    expert_rows = jnp.zeros((EXPERTS * N_EP * CAP, D), jnp.bfloat16).at[slot_index].set(normed[token_index])
    expert_rows = expert_rows.reshape(EXPERTS, N_EP * CAP, D)
    results = lax.map(one_expert, (expert_rows, expert_gate, expert_up, expert_down))
    results = results.reshape(EXPERTS * N_EP * CAP, D)
    picked = results[slot_index].astype(jnp.float32).reshape(TOKENS_M, TOPK, D)
    scores = route_scores.astype(jnp.float32)
    gates = scores / lax.optimization_barrier(jnp.sum(scores, axis=-1, keepdims=True)) * ROUTED_SCALE
    expert_mix = (shared_result + lax.optimization_barrier(jnp.sum(gates[:, :, None] * picked, axis=1))).astype(jnp.bfloat16)
    return (mixed_tokens, expert_mix)
```

```python
import functools

import jax
import jax.numpy as jnp
from jax import lax
from jax.experimental import pallas as pl
from jax.experimental.pallas import tpu as pltpu
from jax.sharding import PartitionSpec as P

MESH = pl.DeviceIdType.MESH
BF = jnp.bfloat16
F32 = jnp.float32
NX, NZ, NY = 4, 8, 8
UP, DOWN = 4, 3
LOG2E = 1.4426950408889634
EPS_NORM = 1e-06
ROUTED_SCALE = 2.5
S = 512
H = 128
KVR = 1040
CAPP = 16
CAP = 12


def dot(a, b):
    return jnp.dot(a, b, preferred_element_type=F32)


def iota(shape, dim):
    return lax.broadcasted_iota(jnp.int32, shape, dim)


def attend(query, key, value, bias, diagonal):
    half = S // 2
    logit = lax.dot_general(query, key, (((1,), (1,)), ((), ())), preferred_element_type=F32)
    logit = logit * (LOG2E / H**0.5) + bias
    soft = jnp.maximum(logit, jnp.log2(1.0 + jnp.exp2(jnp.minimum(logit, 100.0))))
    base = logit - soft
    if diagonal:
        visible = iota(soft.shape, 1) < iota(soft.shape, 0)
        soft = jnp.where(visible, soft, 0.0)
    soft = soft.astype(BF)
    later = jnp.where(iota((half, half), 0) > iota((half, half), 1), 1.0, 0.0).astype(BF)
    stay_hi = dot(soft[:, half:], later)
    sum_hi = stay_hi[:, 0:1] + soft[:, half : half + 1].astype(F32)
    stay_lo = dot(soft[:, :half], later) + sum_hi
    total = stay_lo[:, 0:1] + soft[:, 0:1].astype(F32)
    weight = jnp.exp2(base - jnp.concatenate([stay_lo, stay_hi], axis=1))
    if diagonal:
        weight = jnp.where(visible, weight, 0.0)
    return dot(weight.astype(BF), value), total


def kernel(
    q_in, k_in, v_in, bias_in, ow_in, mi_in, gain, ids, scores, sg_in, su_in, sd_in, eg_in, eu_in, ed_in,
    mixed, mix,
    qb, kvb, op, tcol, tr, ts, osend, orecv, oacc, heads,
    wgu, sgu, ed, sd, ow, mi, normed, gated,
    a1s, a1r, a2r, ag, b0, b1r, b2r, common,
    part_m, sib_m, ring_m, rsend_m, part_a, sib_a, ring_a, rsend_a,
    lsem, q_s, q_r, kv_s, kv_r, a1_s, a1_rs, a2_s, a2_rs, ag_s, ag_r, ags_s, ags_r,
    b1_s, b1_rs, b2_s, b2_rs, t_s, t_r, o_s, o_r,
    msib_s, msib_r, mring_s, mring_r, asib_s, asib_r, aring_s, aring_r,
):
    ep, tp = lax.axis_index("ep"), lax.axis_index("tp")
    z, x, y, c = ep // NX, ep % NX, tp // 2, tp % 2

    def at_x(d):
        return {"ep": z * NX + (x + d) % NX, "tp": tp}

    def at_z(d):
        return {"ep": ((z + d) % NZ) * NX + x, "tp": tp}

    def at_y(d):
        return {"ep": ep, "tp": ((y + d) % NY) * 2 + c}

    sibling = {"ep": ep, "tp": y * 2 + (1 - c)}

    def send(src, dst, ssem, rsem, dev):
        return pltpu.make_async_remote_copy(
            src_ref=src, dst_ref=dst, send_sem=ssem, recv_sem=rsem, device_id=dev, device_id_type=MESH
        )

    local = [
        (q_in, qb.at[x]),
        (k_in, kvb.at[z, 0:S]),
        (v_in, kvb.at[z, S : 2 * S]),
        (bias_in, kvb.at[z, 2 * S : KVR]),
        (mi_in, mi),
        (eg_in, wgu.at[:, 0:H]),
        (eu_in, wgu.at[:, H : 2 * H]),
        (sg_in, sgu.at[:, 0:H]),
        (su_in, sgu.at[:, H : 2 * H]),
        (ed_in, ed),
        (sd_in, sd),
        (ow_in, ow),
    ]
    fetch = [pltpu.make_async_copy(a, b, lsem.at[i]) for i, (a, b) in enumerate(local)]
    for f in fetch:
        f.start()

    barrier = pltpu.get_barrier_semaphore()
    partners = [at_x(d) for d in range(1, NX)] + [at_z(d) for d in range(1, NZ)]
    partners += [at_y(1), at_y(-1), sibling]
    for dev in partners:
        pl.semaphore_signal(barrier, inc=1, device_id=dev, device_id_type=MESH)
    pl.semaphore_wait(barrier, len(partners))

    pending = []

    def begin(copy, when=None):
        pending.append((when, copy))
        if when is None:
            copy.start()
        else:
            pl.when(when)(copy.start)

    def up(d):
        block = kvb.at[jnp.maximum(z - d + 1, 0)]
        return send(block, block, kv_s.at[0, d - 1], kv_r.at[0, d - 1], at_z(1))

    def up_arrival(d):
        block = kvb.at[jnp.maximum(z - d, 0)]
        return send(block, block, kv_s.at[0, d - 1], kv_r.at[0, d - 1], at_z(1))

    def down(d):
        block = kvb.at[(z + d - 1) % NZ]
        return send(block, block, kv_s.at[1, d - 1], kv_r.at[1, d - 1], at_z(-1))

    def down_arrival(d):
        block = kvb.at[(z + d) % NZ]
        return send(block, block, kv_s.at[1, d - 1], kv_r.at[1, d - 1], at_z(-1))

    def step(qi, zi, diagonal):
        key, value = kvb[zi, 0:S, :], kvb[zi, S : 2 * S, :]
        rows = kvb[zi, 2 * S : KVR, :].astype(F32) * LOG2E
        bias = jnp.concatenate([rows[j : j + 1, :] for j in range(S // H)], axis=1)
        out, total = attend(qb[qi], key, value, bias, diagonal)
        op[qi, zi] = out
        tcol[qi] = jnp.where(iota((S, H), 1) == zi, total, tcol[qi])

    def attention():
        fetch[0].wait()
        q_out = [send(qb.at[x], qb.at[x], q_s.at[d - 1], q_r.at[d - 1], at_x(d)) for d in range(1, NX)]
        for cp in q_out:
            begin(cp)
        for f in fetch[1:4]:
            f.wait()
        begin(up(1), z < NZ - 1)
        begin(down(1), z < DOWN)
        tcol[...] = jnp.zeros_like(tcol)
        yield
        step(x, z, True)
        yield
        for d in range(1, NX):
            src = qb.at[(x - d + NX) % NX]
            send(src, src, q_s.at[d - 1], q_r.at[d - 1], at_x(d)).wait_recv()

        def own_row(qi, carry):
            @pl.when(qi > x)
            def _():
                step(qi, z, False)

            @pl.when(qi < x)
            def _():
                op[qi, z] = jnp.zeros((S, H), F32)

            return carry

        lax.fori_loop(0, NX, own_row, 0)
        yield

        def all_rows(zi):
            def one(qi, carry):
                step(qi, zi, False)
                return carry

            lax.fori_loop(0, NX, one, 0)

        for d in range(1, UP + 1):

            @pl.when(z >= d)
            def _():
                up_arrival(d).wait_recv()

            if d < UP:
                begin(up(d + 1), (z >= d) & (z < NZ - 1))
            if d <= DOWN:
                came = (z + d) % NZ

                @pl.when(came < DOWN)
                def _():
                    down_arrival(d).wait_recv()

                if d < DOWN:
                    begin(down(d + 1), came < DOWN)

            @pl.when(z >= d)
            def _():
                all_rows(jnp.maximum(z - d, 0))

            yield
            if d <= DOWN:

                @pl.when((came < DOWN) & (came < z))
                def _():
                    all_rows(came)

                yield
        for qi in range(NX):
            ts[qi] = tcol[qi].T[0:NZ, :]
        for d in range(1, NX):
            begin(send(ts, tr.at[x], t_s.at[d - 1], t_r.at[d - 1], at_x(d)))
        tr[x] = ts[...]
        yield
        for d in range(1, NX):
            src = tr.at[(x - d + NX) % NX]
            send(ts, src, t_s.at[d - 1], t_r.at[d - 1], at_x(d)).wait_recv()

        def combine(qi):
            sums = [tr[i, qi] for i in range(NX)]
            row = sums[0] + sums[1] + sums[2] + sums[3]
            within = sum(jnp.where(i > x, sums[i], 0.0) for i in range(1, NX))
            parts, run = [], jnp.zeros((1, S), F32)
            for zi in reversed(range(NZ)):
                parts.append(run)
                run = run + row[zi : zi + 1, :]
            carried = jnp.concatenate(parts[::-1], axis=0) + within
            scale = jnp.exp2(-carried)
            scale = jnp.concatenate([scale, jnp.zeros((H - NZ, S), F32)], axis=0).T
            for zi in range(NZ):
                if zi == 0:
                    oacc[...] = scale[:, 0:1] * op[qi, 0]
                else:

                    @pl.when(zi <= z)
                    def _():
                        oacc[...] += scale[:, zi : zi + 1] * op[qi, zi]

        for d in range(1, NX):
            qi = (x + d) % NX
            combine(qi)
            osend[d - 1] = oacc[...].astype(BF)
            begin(send(osend.at[d - 1], orecv.at[d - 1], o_s.at[d - 1], o_r.at[d - 1], at_x(d)))
        combine(x)
        yield
        for d in range(1, NX):
            send(osend.at[d - 1], orecv.at[d - 1], o_s.at[d - 1], o_r.at[d - 1], at_x(d)).wait_recv()
        total = oacc[...]
        for d in range(1, NX):
            total = total + orecv[d - 1].astype(F32)
        heads[...] = total.astype(BF)
        fetch[11].wait()
        for yi in range(NY):
            both = dot(heads[...], ow[:, yi * 256 : (yi + 1) * 256]).astype(BF)
            part_a[0, yi] = both[:, :H]
            part_a[1, yi] = both[:, H:]
        out = yield from reduce_scatter(part_a, sib_a, ring_a, rsend_a, asib_s, asib_r, aring_s, aring_r)
        mixed[...] = out.astype(BF)

    def reduce_scatter(part, sib, ring, rsend, sib_s, sib_r, ring_s, ring_r):
        order = [4, -3, 3, -2, 2, -1, 1, 0]

        def to_sibling(m):
            yi = (y + order[m] + NY) % NY
            return send(part.at[1 - c, yi], sib.at[m], sib_s.at[m], sib_r.at[m], sibling)

        for m in range(NY):
            begin(to_sibling(m))
        yield

        def mine(m):
            to_sibling(m).wait_recv()
            yi = (y + order[m] + NY) % NY
            return part[c, yi].astype(F32) + sib[m].astype(F32)

        def hop(way, s):
            return send(
                rsend.at[way, s], ring.at[way, s], ring_s.at[way, s], ring_r.at[way, s], at_y(1 - 2 * way)
            )

        for s in range(4):
            for way in range(2):
                if way == 1 and s == 3:
                    continue
                value = mine(2 * s + way)
                if s > 0:
                    hop(way, s - 1).wait_recv()
                    value = value + ring[way, s - 1].astype(F32)
                rsend[way, s] = value.astype(BF)
                begin(hop(way, s))
            yield
        value = mine(7)
        hop(1, 2).wait_recv()
        value = value + ring[1, 2].astype(F32)
        hop(0, 3).wait_recv()
        return value + ring[0, 3].astype(F32)

    def spread(transposed):
        shape = (NZ * NX * CAPP, NZ * NX * CAP) if transposed else (NZ * NX * CAP, NZ * NX * CAPP)
        padded, packed = (iota(shape, 0), iota(shape, 1)) if transposed else (iota(shape, 1), iota(shape, 0))
        place = padded & (CAPP - 1)
        hit = ((padded >> 4) * CAP + place == packed) & (place < CAP)
        return jnp.where(hit, 1.0, 0.0).astype(BF)

    def experts():
        fetch[4].wait()
        value = mi[...].astype(F32)
        mean = jnp.mean(value * value, axis=1, keepdims=True)
        normed[...] = (value * lax.rsqrt(mean + EPS_NORM) * gain[...]).astype(BF)
        own = normed[:, pl.ds(pl.multiple_of(tp * H, H), H)]
        slots = NZ * NX * CAPP
        group = iota((slots, 128), 0) >> 4
        place = iota((slots, 128), 0) & (CAPP - 1)
        expert = (group & (NZ - 1)) * NX + (group >> 3)
        first, second = ids[0:1, :] == expert, ids[1:2, :] == expert
        named = first | second
        earlier = jnp.where(iota((128, 128), 0) < iota((128, 128), 1), 1.0, 0.0).astype(BF)
        count = dot(jnp.where(named, 1.0, 0.0).astype(BF), earlier)
        chosen = named & (count == place.astype(F32))
        scale = ROUTED_SCALE / (scores[0:1, :] + scores[1:2, :])
        gate = jnp.where(first, scores[0:1, :] * scale, 0.0) + jnp.where(second, scores[1:2, :] * scale, 0.0)
        gated[...] = jnp.where(chosen, gate, 0.0)
        out = dot(jnp.where(chosen, 1.0, 0.0).astype(BF), own).astype(BF)
        a1s[...] = out.reshape(NX, NZ, CAPP, H)

        def by_x(d):
            return send(a1s.at[(x + d) % NX], a1r.at[x], a1_s.at[d - 1], a1_rs.at[d - 1], at_x(d))

        for d in range(1, NX):
            begin(by_x(d))
        a1r[x] = a1s[x]
        yield
        for d in range(1, NX):
            send(a1s.at[x], a1r.at[(x - d + NX) % NX], a1_s.at[d - 1], a1_rs.at[d - 1], at_x(d)).wait_recv()
        for d in range(1, NZ):
            begin(send(a1r.at[:, (z + d) % NZ], a2r.at[z], a2_s.at[d - 1], a2_rs.at[d - 1], at_z(d)))
        a2r[z] = a1r[:, z]
        yield
        for d in range(1, NZ):
            send(a1r.at[:, z], a2r.at[(z - d + NZ) % NZ], a2_s.at[d - 1], a2_rs.at[d - 1], at_z(d)).wait_recv()
        packed = dot(spread(False), a2r[...].reshape(slots, H)).astype(BF)
        ag[tp] = packed

        def along(way, s):
            sign = 1 - 2 * way
            mine = ag.at[((y - sign * (s - 1) + NY) % NY) * 2 + c]
            return send(mine, mine, ag_s.at[way, s - 1], ag_r.at[way, s - 1], at_y(sign))

        def arrival(way, s):
            sign = 1 - 2 * way
            theirs = ag.at[((y - sign * s + NY) % NY) * 2 + c]
            return send(theirs, theirs, ag_s.at[way, s - 1], ag_r.at[way, s - 1], at_y(sign))

        def across(m, yi, core):
            ref = ag.at[yi * 2 + core]
            return send(ref, ref, ags_s.at[m], ags_r.at[m], sibling)

        begin(along(0, 1))
        begin(along(1, 1))
        begin(across(0, y, c))
        yield
        for s in range(1, 5):
            for way in range(2):
                if way == 1 and s == 4:
                    continue
                arrival(way, s).wait_recv()
                if s < 4 - way:
                    begin(along(way, s + 1))
                sign = 1 - 2 * way
                begin(across(way * 4 + s, (y - sign * s + NY) % NY, c))
            yield
        across(0, y, 1 - c).wait_recv()
        for s in range(1, 5):
            for way in range(2):
                if way == 1 and s == 4:
                    continue
                sign = 1 - 2 * way
                across(way * 4 + s, (y - sign * s + NY) % NY, 1 - c).wait_recv()
        for i in (5, 6, 7, 8, 9, 10):
            fetch[i].wait()
        acc = jnp.zeros((NZ * NX * CAP, 2 * H), F32)
        acc_s = jnp.zeros((128, 2 * H), F32)
        for j in range(NY):
            wide = jnp.concatenate([ag[2 * j], ag[2 * j + 1]], axis=1)
            acc = acc + dot(wide, wgu[j * 256 : (j + 1) * 256, :])
            acc_s = acc_s + dot(normed[:, j * 256 : (j + 1) * 256], sgu[j * 256 : (j + 1) * 256, :])

        def swiglu(a):
            g, u = a[:, :H], a[:, H:]
            return (g / (1.0 + jnp.exp(-g)) * u).astype(BF)

        hidden, hidden_s = swiglu(acc), swiglu(acc_s)
        rows = NZ * NX * CAP
        for yi in range(NY):
            cols = slice(yi * 256, (yi + 1) * 256)
            both = dot(hidden, ed[:, cols]).astype(BF)
            part_m[0, yi, 0:rows] = both[:, :H]
            part_m[1, yi, 0:rows] = both[:, H:]
            both = dot(hidden_s, sd[:, cols]).astype(BF)
            part_m[0, yi, rows:S] = both[:, :H]
            part_m[1, yi, rows:S] = both[:, H:]
        out = yield from reduce_scatter(part_m, sib_m, ring_m, rsend_m, msib_s, msib_r, mring_s, mring_r)
        common[...] = out[rows:S, :]
        b0[...] = dot(spread(True), out[0:rows, :].astype(BF)).astype(BF).reshape(NZ, NX, CAPP, H)
        for d in range(1, NZ):
            begin(send(b0.at[(z + d) % NZ], b1r.at[z], b1_s.at[d - 1], b1_rs.at[d - 1], at_z(d)))
        b1r[z] = b0[z]
        yield
        for d in range(1, NZ):
            send(b0.at[z], b1r.at[(z - d + NZ) % NZ], b1_s.at[d - 1], b1_rs.at[d - 1], at_z(d)).wait_recv()
        for d in range(1, NX):
            begin(send(b1r.at[:, (x + d) % NX], b2r.at[x], b2_s.at[d - 1], b2_rs.at[d - 1], at_x(d)))
        b2r[x] = b1r[:, x]
        yield
        for d in range(1, NX):
            send(b1r.at[:, x], b2r.at[(x - d + NX) % NX], b2_s.at[d - 1], b2_rs.at[d - 1], at_x(d)).wait_recv()
        gates = gated[...].T
        high = gates.astype(BF)
        low = (gates - high.astype(F32)).astype(BF)
        got = b2r[...].reshape(slots, H)
        mix[...] = (common[...] + dot(high, got) + dot(low, got)).astype(BF)

    def advance(work):
        try:
            next(work)
            return True
        except StopIteration:
            return False

    attn, moe = attention(), experts()
    live = [True, True]
    while any(live):
        live[0] = live[0] and advance(attn)
        live[1] = live[1] and advance(moe)

    for when, copy in pending:
        if when is None:
            copy.wait_send()
        else:
            pl.when(when)(copy.wait_send)


def body(
    queries, keys, values, key_bias, out_weight, moe_input, moe_gain, route_ids, route_scores,
    shared_gate, shared_up, shared_down, expert_gate, expert_up, expert_down,
):
    bias = jnp.pad(key_bias.reshape(S // H, H), ((0, KVR - 2 * S - S // H), (0, 0)))
    ids = jnp.pad(route_ids.T, ((0, 6), (0, 0)))
    scores = jnp.pad(route_scores.T, ((0, 6), (0, 0)))
    hbm, vmem = pl.BlockSpec(memory_space=pl.ANY), pl.BlockSpec(memory_space=pltpu.VMEM)
    dma = pltpu.SemaphoreType.DMA
    V = pltpu.VMEM
    slots = (NZ, NX, CAPP, H)
    rs = [V((2, NY, S, H), BF), V((NY, S, H), BF), V((2, 4, S, H), BF), V((2, 4, S, H), BF)]
    sems = [dma((12,)), dma((3,)), dma((3,)), dma((2, 4)), dma((2, 4)), dma((3,)), dma((3,)), dma((7,)), dma((7,))]
    sems += [dma((2, 4)), dma((2, 4)), dma((8,)), dma((8,))]
    sems += [dma((7,)), dma((7,)), dma((3,)), dma((3,)), dma((3,)), dma((3,)), dma((3,)), dma((3,))]
    sems += [dma((8,)), dma((8,)), dma((2, 4)), dma((2, 4))] * 2
    return pl.pallas_call(
        kernel,
        out_shape=(jax.ShapeDtypeStruct((S, H), BF), jax.ShapeDtypeStruct((128, H), BF)),
        in_specs=[hbm] * 6 + [vmem] * 3 + [hbm] * 6,
        out_specs=(vmem, vmem),
        scratch_shapes=[
            V((NX, S, H), BF), V((NZ, KVR, H), BF), V((NX, NZ, S, H), F32), V((NX, S, H), F32),
            V((NX, NX, NZ, S), F32), V((NX, NZ, S), F32), V((NX - 1, S, H), BF), V((NX - 1, S, H), BF),
            V((S, H), F32), V((S, H), BF),
            V((2048, 2 * H), BF), V((2048, 2 * H), BF), V((H, 2048), BF), V((H, 2048), BF), V((H, 2048), BF),
            V((128, 2048), BF), V((128, 2048), BF), V((512, 128), F32),
            V((NX, NZ, CAPP, H), BF), V((NX, NZ, CAPP, H), BF), V(slots, BF), V((16, NZ * NX * CAP, H), BF),
            V(slots, BF), V(slots, BF), V((NX, NZ, CAPP, H), BF), V((128, H), F32),
            *rs, *rs, *sems,
        ],
        compiler_params=pltpu.CompilerParams(
            collective_id=0, has_side_effects=True, vmem_limit_bytes=60 * 2**20
        ),
        name="fused",
    )(
        queries, keys, values, bias, out_weight, moe_input, moe_gain.reshape(1, -1), ids, scores,
        shared_gate, shared_up, shared_down,
        expert_gate.reshape(2048, H), expert_up.reshape(2048, H), expert_down.reshape(H, 2048),
    )


def solution(mesh):
    return jax.shard_map(
        body,
        mesh=mesh,
        in_specs=(
            P("ep", "tp"), P("ep", "tp"), P("ep", "tp"), P("ep", "tp"), P("tp", None), P("ep", None), P(),
            P("ep", None), P("ep", None), P(None, "tp"), P(None, "tp"), P("tp", None),
            P("ep", None, "tp"), P("ep", None, "tp"), P("ep", "tp", None),
        ),
        out_specs=(P("ep", "tp"), P("ep", "tp")),
        check_vma=False,
    )
```

```python
import functools

import jax
import jax.numpy as jnp
from jax import lax
from jax.experimental import pallas as pl
from jax.experimental.pallas import tpu as pltpu
from jax.sharding import PartitionSpec as P

MESH = pl.DeviceIdType.MESH
BF = jnp.bfloat16
F32 = jnp.float32
NX, NZ, NY = 4, 8, 8
UP, DOWN = 4, 3
LOG2E = 1.4426950408889634
EPS_NORM = 1e-06
ROUTED_SCALE = 2.5
S = 512
H = 128
KB = 528
KVR = 1040
CAPP = 16
CAP = 12


def dot(a, b):
    return jnp.dot(a, b, preferred_element_type=F32)


def iota(shape, dim):
    return lax.broadcasted_iota(jnp.int32, shape, dim)


def attend(query, key, value, bias, first):
    half = S // 2
    logit = lax.dot_general(query, key, (((1,), (1,)), ((), ())), preferred_element_type=F32)
    logit = logit * (LOG2E / H**0.5) + bias
    soft = jnp.maximum(logit, jnp.log2(1.0 + jnp.exp2(jnp.minimum(logit, 100.0))))
    base = logit - soft
    if first is not None:
        visible = iota(soft.shape, 1) + first < iota(soft.shape, 0)
        soft = jnp.where(visible, soft, 0.0)
    soft = soft.astype(BF)
    later = jnp.where(iota((half, half), 0) > iota((half, half), 1), 1.0, 0.0).astype(BF)
    stay_hi = dot(soft[:, half:], later)
    sum_hi = stay_hi[:, 0:1] + soft[:, half : half + 1].astype(F32)
    stay_lo = dot(soft[:, :half], later) + sum_hi
    total = stay_lo[:, 0:1] + soft[:, 0:1].astype(F32)
    weight = jnp.exp2(base - jnp.concatenate([stay_lo, stay_hi], axis=1))
    if first is not None:
        weight = jnp.where(visible, weight, 0.0)
    return dot(weight.astype(BF), value), total


def kernel(
    q_in, k_in, v_in, bias_in, ow_in, mi_in, gain_in, ids_in, scores_in, sg_in, su_in, sd_in, eg_in, eu_in, ed_in,
    mixed, mix,
    qb, kvb, op, tcol, tr, ts, osend, orecv, oacc, heads,
    bias, gain, ids, scores, wgu, sgu, ed, sd, ow, mi, normed, gated,
    a1s, a1r, a2r, ag, b0, b1r, b2r, common,
    part_m, sib_m, ring_m, rsend_m, part_a, sib_a, ring_a, rsend_a,
    lsem, q_s, q_r, kv_s, kv_r, a1_s, a1_rs, a2_s, a2_rs, ag_s, ag_r, ags_s, ags_r,
    b1_s, b1_rs, b2_s, b2_rs, t_s, t_r, o_s, o_r,
    msib_s, msib_r, mring_s, mring_r, asib_s, asib_r, aring_s, aring_r,
):
    ep, tp = lax.axis_index("ep"), lax.axis_index("tp")
    z, x, y, c = ep // NX, ep % NX, tp // 2, tp % 2

    def at_x(d):
        return {"ep": z * NX + (x + d) % NX, "tp": tp}

    def at_z(d):
        return {"ep": ((z + d) % NZ) * NX + x, "tp": tp}

    def at_y(d):
        return {"ep": ep, "tp": ((y + d) % NY) * 2 + c}

    sibling = {"ep": ep, "tp": y * 2 + (1 - c)}

    def send(src, dst, ssem, rsem, dev):
        return pltpu.make_async_remote_copy(
            src_ref=src, dst_ref=dst, send_sem=ssem, recv_sem=rsem, device_id=dev, device_id_type=MESH
        )

    local = [
        (q_in, qb.at[pl.ds(pl.multiple_of(x * S, S), S)]),
        (k_in, kvb.at[z, 0:S]),
        (v_in, kvb.at[z, KB:KVR]),
        (bias_in, bias),
        (mi_in, mi),
        (eg_in, wgu.at[:, 0:H]),
        (eu_in, wgu.at[:, H : 2 * H]),
        (sg_in, sgu.at[:, 0:H]),
        (su_in, sgu.at[:, H : 2 * H]),
        (ed_in, ed),
        (sd_in, sd),
        (ow_in, ow),
        (gain_in, gain),
        (ids_in, ids),
        (scores_in, scores),
    ]
    fetch = [pltpu.make_async_copy(a, b, lsem.at[i]) for i, (a, b) in enumerate(local)]

    barrier = pltpu.get_barrier_semaphore()
    partners = [at_x(d) for d in range(1, NX)] + [at_z(d) for d in range(1, NZ)]
    partners += [at_y(1), at_y(-1), sibling]
    for dev in partners:
        pl.semaphore_signal(barrier, inc=1, device_id=dev, device_id_type=MESH)
    for i in (4, 12, 13, 14, 3, 0, 1, 2, 5, 6, 7, 8, 9, 10, 11):
        fetch[i].start()

    pending = []

    def begin(copy, when=None):
        pending.append((when, copy))
        if when is None:
            copy.start()
        else:
            pl.when(when)(copy.start)

    halves = (slice(0, KB), slice(KB, KVR))

    def query_rows(i):
        return qb.at[pl.ds(pl.multiple_of(i * S, S), S)]

    def up(d, h):
        block = kvb.at[jnp.maximum(z - d + 1, 0), halves[h]]
        return send(block, block, kv_s.at[0, d - 1, h], kv_r.at[0, d - 1, h], at_z(1))

    def up_arrival(d, h):
        block = kvb.at[jnp.maximum(z - d, 0), halves[h]]
        return send(block, block, kv_s.at[0, d - 1, h], kv_r.at[0, d - 1, h], at_z(1))

    def down(d, h):
        block = kvb.at[(z + d - 1) % NZ, halves[h]]
        return send(block, block, kv_s.at[1, d - 1, h], kv_r.at[1, d - 1, h], at_z(-1))

    def down_arrival(d, h):
        block = kvb.at[(z + d) % NZ, halves[h]]
        return send(block, block, kv_s.at[1, d - 1, h], kv_r.at[1, d - 1, h], at_z(-1))

    def step(zi, first):
        rows = kvb[zi, S:KB, :].astype(F32) * LOG2E
        row = jnp.concatenate([rows[j : j + 1, :] for j in range(S // H)], axis=1)
        out, total = attend(qb[...], kvb[zi, 0:S, :], kvb[zi, KB:KVR, :], row, first)
        op[zi] = out
        tcol[...] = jnp.where(iota((NX * S, H), 1) == zi, total, tcol[...])

    def attention():
        fetch[0].wait()
        for d in range(1, NX):
            begin(send(query_rows(x), query_rows(x), q_s.at[d - 1], q_r.at[d - 1], at_x(d)))
        fetch[1].wait()
        begin(up(1, 0), z < NZ - 1)
        begin(down(1, 0), z < DOWN)
        yield
        fetch[2].wait()
        begin(up(1, 1), z < NZ - 1)
        begin(down(1, 1), z < DOWN)
        tcol[...] = jnp.zeros_like(tcol)
        for d in range(1, NX):
            src = query_rows((x - d + NX) % NX)
            send(src, src, q_s.at[d - 1], q_r.at[d - 1], at_x(d)).wait_recv()
        step(z, x * S)
        yield
        for d in range(1, UP + 1):
            came = (z + d) % NZ
            for h in range(2):

                @pl.when(z >= d)
                def _():
                    up_arrival(d, h).wait_recv()

                if d < UP:
                    begin(up(d + 1, h), (z >= d) & (z < NZ - 1))
                if d <= DOWN:

                    @pl.when(came < DOWN)
                    def _():
                        down_arrival(d, h).wait_recv()

                    if d < DOWN:
                        begin(down(d + 1, h), came < DOWN)

            @pl.when(z >= d)
            def _():
                step(jnp.maximum(z - d, 0), None)

            yield
            if d <= DOWN:

                @pl.when((came < DOWN) & (came < z))
                def _():
                    step(came, None)

                yield
        for qi in range(NX):
            ts[qi] = tcol[qi * S : (qi + 1) * S].T[0:NZ, :]
        for d in range(1, NX):
            begin(send(ts, tr.at[x], t_s.at[d - 1], t_r.at[d - 1], at_x(d)))
        tr[x] = ts[...]
        yield
        for d in range(1, NX):
            src = tr.at[(x - d + NX) % NX]
            send(ts, src, t_s.at[d - 1], t_r.at[d - 1], at_x(d)).wait_recv()

        def combine(qi):
            sums = [tr[i, qi] for i in range(NX)]
            row = sums[0] + sums[1] + sums[2] + sums[3]
            within = sum(jnp.where(i > x, sums[i], 0.0) for i in range(1, NX))
            parts, run = [], jnp.zeros((1, S), F32)
            for zi in reversed(range(NZ)):
                parts.append(run)
                run = run + row[zi : zi + 1, :]
            carried = jnp.concatenate(parts[::-1], axis=0) + within
            scale = jnp.exp2(-carried)
            scale = jnp.concatenate([scale, jnp.zeros((H - NZ, S), F32)], axis=0).T
            rows = pl.ds(pl.multiple_of(qi * S, S), S)
            oacc[...] = scale[:, 0:1] * op[0, rows, :]
            for zi in range(1, NZ):

                @pl.when(zi <= z)
                def _():
                    oacc[...] += scale[:, zi : zi + 1] * op[zi, rows, :]

        for d in range(1, NX):
            qi = (x + d) % NX
            combine(qi)
            osend[d - 1] = oacc[...].astype(BF)
            begin(send(osend.at[d - 1], orecv.at[d - 1], o_s.at[d - 1], o_r.at[d - 1], at_x(d)))
        combine(x)
        yield
        for d in range(1, NX):
            send(osend.at[d - 1], orecv.at[d - 1], o_s.at[d - 1], o_r.at[d - 1], at_x(d)).wait_recv()
        total = oacc[...]
        for d in range(1, NX):
            total = total + orecv[d - 1].astype(F32)
        heads[...] = total.astype(BF)
        fetch[11].wait()

        def fill(yi):
            both = dot(heads[...], ow[:, pl.ds(pl.multiple_of(yi * 256, 256), 256)]).astype(BF)
            part_a[0, yi] = both[:, :H]
            part_a[1, yi] = both[:, H:]

        out = yield from reduce_scatter(
            fill, 2, part_a, sib_a, ring_a, rsend_a, asib_s, asib_r, aring_s, aring_r
        )
        mixed[...] = out.astype(BF)

    def reduce_scatter(fill, cuts, part, sib, ring, rsend, sib_s, sib_r, ring_s, ring_r):
        order = [4, -3, 3, -2, 2, -1, 1, 0]
        length = S // cuts
        spans = [slice(i * length, (i + 1) * length) for i in range(cuts)]

        def to_sibling(m):
            yi = (y + order[m] + NY) % NY
            return send(part.at[1 - c, yi], sib.at[m], sib_s.at[m], sib_r.at[m], sibling)

        for m in range(NY):
            fill((y + order[m] + NY) % NY)
            begin(to_sibling(m))
        yield

        def mine(m, span):
            yi = (y + order[m] + NY) % NY
            return part[c, yi, span].astype(F32) + sib[m, span].astype(F32)

        def hop(way, s, i):
            return send(
                rsend.at[way, s, spans[i]], ring.at[way, s, spans[i]],
                ring_s.at[way, s, i], ring_r.at[way, s, i], at_y(1 - 2 * way),
            )

        for s in range(4):
            for i in range(cuts):
                for way in range(2):
                    if way == 1 and s == 3:
                        continue
                    if i == 0:
                        to_sibling(2 * s + way).wait_recv()
                    value = mine(2 * s + way, spans[i])
                    if s > 0:
                        hop(way, s - 1, i).wait_recv()
                        value = value + ring[way, s - 1, spans[i]].astype(F32)
                    rsend[way, s, spans[i]] = value.astype(BF)
                    begin(hop(way, s, i))
            yield
        to_sibling(7).wait_recv()
        done = []
        for i in range(cuts):
            value = mine(7, spans[i])
            hop(1, 2, i).wait_recv()
            value = value + ring[1, 2, spans[i]].astype(F32)
            hop(0, 3, i).wait_recv()
            done.append(value + ring[0, 3, spans[i]].astype(F32))
        return jnp.concatenate(done, axis=0) if cuts > 1 else done[0]

    def spread(transposed):
        shape = (NZ * NX * CAPP, NZ * NX * CAP) if transposed else (NZ * NX * CAP, NZ * NX * CAPP)
        padded, packed = (iota(shape, 0), iota(shape, 1)) if transposed else (iota(shape, 1), iota(shape, 0))
        place = padded & (CAPP - 1)
        hit = ((padded >> 4) * CAP + place == packed) & (place < CAP)
        return jnp.where(hit, 1.0, 0.0).astype(BF)

    def experts():
        for i in (4, 12, 13, 14):
            fetch[i].wait()
        value = mi[...].astype(F32)
        mean = jnp.mean(value * value, axis=1, keepdims=True)
        normed[...] = (value * lax.rsqrt(mean + EPS_NORM) * gain[...]).astype(BF)
        facing = ((y + NY // 2) % NY) * 2 + c
        own = jnp.concatenate([normed[:, pl.ds(pl.multiple_of(i * H, H), H)] for i in (tp, facing)], axis=1)
        slots = NZ * NX * CAPP
        group = iota((slots, 128), 0) >> 4
        place = iota((slots, 128), 0) & (CAPP - 1)
        expert = (group & (NZ - 1)) * NX + (group >> 3)
        first, second = ids[0:1, :] == expert, ids[1:2, :] == expert
        named = first | second
        earlier = jnp.where(iota((128, 128), 0) < iota((128, 128), 1), 1.0, 0.0).astype(BF)
        count = dot(jnp.where(named, 1.0, 0.0).astype(BF), earlier)
        chosen = named & (count == place.astype(F32))
        scale = ROUTED_SCALE / (scores[0:1, :] + scores[1:2, :])
        gate = jnp.where(first, scores[0:1, :] * scale, 0.0) + jnp.where(second, scores[1:2, :] * scale, 0.0)
        gated[...] = jnp.where(chosen, gate, 0.0)
        out = dot(jnp.where(chosen, 1.0, 0.0).astype(BF), own).astype(BF)
        a1s[...] = out.reshape(NX, NZ, CAPP, 2 * H)
        fetch[3].wait()
        line = bias[...]
        line = [line[:, j * H : (j + 1) * H] for j in range(S // H)]
        kvb[z, S:KB, :] = jnp.concatenate(line + [jnp.zeros((KB - S - S // H, H), BF)], axis=0)
        pl.semaphore_wait(barrier, len(partners))

        def by_x(d):
            return send(a1s.at[(x + d) % NX], a1r.at[x], a1_s.at[d - 1], a1_rs.at[d - 1], at_x(d))

        for d in range(1, NX):
            begin(by_x(d))
        a1r[x] = a1s[x]
        yield
        for d in range(1, NX):
            send(a1s.at[x], a1r.at[(x - d + NX) % NX], a1_s.at[d - 1], a1_rs.at[d - 1], at_x(d)).wait_recv()
        for d in range(1, NZ):
            begin(send(a1r.at[:, (z + d) % NZ], a2r.at[z], a2_s.at[d - 1], a2_rs.at[d - 1], at_z(d)))
        a2r[z] = a1r[:, z]
        yield
        for d in range(1, NZ):
            send(a1r.at[:, z], a2r.at[(z - d + NZ) % NZ], a2_s.at[d - 1], a2_rs.at[d - 1], at_z(d)).wait_recv()
        packed = dot(spread(False), a2r[...].reshape(slots, 2 * H)).astype(BF)
        ag[tp] = packed[:, :H]
        ag[facing] = packed[:, H:]

        def slice_of(yi, core=c):
            return ag.at[((yi + NY) % NY) * 2 + core]

        def along(way, n, yi):
            return send(slice_of(yi), slice_of(yi), ag_s.at[way, n], ag_r.at[way, n], at_y(1 - 2 * way))

        def across(m, yi, core):
            return send(slice_of(yi, core), slice_of(yi, core), ags_s.at[m], ags_r.at[m], sibling)

        for n in range(2):
            for way in range(2):
                begin(along(way, n, y + n * NY // 2))
        begin(across(0, y, c))
        begin(across(1, y + NY // 2, c))
        yield
        for way in range(2):
            near = y - (1 - 2 * way)
            along(way, 0, near).wait_recv()
            begin(along(way, 2, near))
            begin(across(2 + way, near, c))
        yield
        for n in range(1, 3):
            for way in range(2):
                sign = 1 - 2 * way
                came = y - sign + NY // 2 if n == 1 else y - 2 * sign
                along(way, n, came).wait_recv()
                begin(across(2 + 2 * n + way, came, c))
        yield
        across(0, y, 1 - c).wait_recv()
        across(1, y + NY // 2, 1 - c).wait_recv()
        for way in range(2):
            sign = 1 - 2 * way
            across(2 + way, y - sign, 1 - c).wait_recv()
            across(4 + way, y - sign + NY // 2, 1 - c).wait_recv()
            across(6 + way, y - 2 * sign, 1 - c).wait_recv()
        for i in (5, 6, 7, 8, 9, 10):
            fetch[i].wait()
        acc = jnp.zeros((NZ * NX * CAP, 2 * H), F32)
        acc_s = jnp.zeros((128, 2 * H), F32)
        for j in range(NY):
            wide = jnp.concatenate([ag[2 * j], ag[2 * j + 1]], axis=1)
            acc = acc + dot(wide, wgu[j * 256 : (j + 1) * 256, :])
            acc_s = acc_s + dot(normed[:, j * 256 : (j + 1) * 256], sgu[j * 256 : (j + 1) * 256, :])

        def swiglu(a):
            g, u = a[:, :H], a[:, H:]
            return (g / (1.0 + jnp.exp(-g)) * u).astype(BF)

        hidden, hidden_s = swiglu(acc), swiglu(acc_s)
        rows = NZ * NX * CAP

        def fill(yi):
            cols = pl.ds(pl.multiple_of(yi * 256, 256), 256)
            both = dot(hidden, ed[:, cols]).astype(BF)
            part_m[0, yi, 0:rows] = both[:, :H]
            part_m[1, yi, 0:rows] = both[:, H:]
            both = dot(hidden_s, sd[:, cols]).astype(BF)
            part_m[0, yi, rows:S] = both[:, :H]
            part_m[1, yi, rows:S] = both[:, H:]

        out = yield from reduce_scatter(
            fill, 1, part_m, sib_m, ring_m, rsend_m, msib_s, msib_r, mring_s, mring_r
        )
        common[...] = out[rows:S, :]
        b0[...] = dot(spread(True), out[0:rows, :].astype(BF)).astype(BF).reshape(NZ, NX, CAPP, H)
        for d in range(1, NZ):
            begin(send(b0.at[(z + d) % NZ], b1r.at[z], b1_s.at[d - 1], b1_rs.at[d - 1], at_z(d)))
        b1r[z] = b0[z]
        yield
        for d in range(1, NZ):
            send(b0.at[z], b1r.at[(z - d + NZ) % NZ], b1_s.at[d - 1], b1_rs.at[d - 1], at_z(d)).wait_recv()
        for d in range(1, NX):
            begin(send(b1r.at[:, (x + d) % NX], b2r.at[x], b2_s.at[d - 1], b2_rs.at[d - 1], at_x(d)))
        b2r[x] = b1r[:, x]
        yield
        for d in range(1, NX):
            send(b1r.at[:, x], b2r.at[(x - d + NX) % NX], b2_s.at[d - 1], b2_rs.at[d - 1], at_x(d)).wait_recv()
        gates = gated[...].T
        high = gates.astype(BF)
        low = (gates - high.astype(F32)).astype(BF)
        got = b2r[...].reshape(slots, H)
        mix[...] = (common[...] + dot(high, got) + dot(low, got)).astype(BF)

    attn, moe = attention(), experts()
    for turn in "mamamaamaamamamaamamaamamamama":
        next(attn if turn == "a" else moe, None)

    for when, copy in pending:
        if when is None:
            copy.wait_send()
        else:
            pl.when(when)(copy.wait_send)


def body(
    queries, keys, values, key_bias, out_weight, moe_input, moe_gain, route_ids, route_scores,
    shared_gate, shared_up, shared_down, expert_gate, expert_up, expert_down,
):
    hbm, vmem = pl.BlockSpec(memory_space=pl.ANY), pl.BlockSpec(memory_space=pltpu.VMEM)
    dma = pltpu.SemaphoreType.DMA
    V = pltpu.VMEM
    slots = (NZ, NX, CAPP, H)
    rs = [V((2, NY, S, H), BF), V((NY, S, H), BF), V((2, 4, S, H), BF), V((2, 4, S, H), BF)]
    sems = [dma((15,)), dma((3,)), dma((3,)), dma((2, 4, 2)), dma((2, 4, 2)), dma((3,)), dma((3,)), dma((7,)), dma((7,))]
    sems += [dma((2, 4)), dma((2, 4)), dma((8,)), dma((8,))]
    sems += [dma((7,)), dma((7,)), dma((3,)), dma((3,)), dma((3,)), dma((3,)), dma((3,)), dma((3,))]
    sems += [dma((8,)), dma((8,)), dma((2, 4, 2)), dma((2, 4, 2))] * 2
    return pl.pallas_call(
        kernel,
        out_shape=(jax.ShapeDtypeStruct((S, H), BF), jax.ShapeDtypeStruct((128, H), BF)),
        in_specs=[hbm] * 15,
        out_specs=(vmem, vmem),
        scratch_shapes=[
            V((NX * S, H), BF), V((NZ, KVR, H), BF), V((NZ, NX * S, H), F32), V((NX * S, H), F32),
            V((NX, NX, NZ, S), F32), V((NX, NZ, S), F32), V((NX - 1, S, H), BF), V((NX - 1, S, H), BF),
            V((S, H), F32), V((S, H), BF),
            V((1, S), BF), V((1, 2048), F32), V((2, 128), jnp.int32), V((2, 128), F32),
            V((2048, 2 * H), BF), V((2048, 2 * H), BF), V((H, 2048), BF), V((H, 2048), BF), V((H, 2048), BF),
            V((128, 2048), BF), V((128, 2048), BF), V((512, 128), F32),
            V((NX, NZ, CAPP, 2 * H), BF), V((NX, NZ, CAPP, 2 * H), BF), V((NZ, NX, CAPP, 2 * H), BF), V((16, NZ * NX * CAP, H), BF),
            V(slots, BF), V(slots, BF), V((NX, NZ, CAPP, H), BF), V((128, H), F32),
            *rs, *rs, *sems,
        ],
        compiler_params=pltpu.CompilerParams(
            collective_id=0, has_side_effects=True, vmem_limit_bytes=60 * 2**20
        ),
        name="fused",
    )(
        queries, keys, values, key_bias.T, out_weight, moe_input, moe_gain.reshape(1, -1), route_ids.T, route_scores.T,
        shared_gate, shared_up, shared_down,
        expert_gate.reshape(2048, H), expert_up.reshape(2048, H), expert_down.reshape(H, 2048),
    )


def solution(mesh):
    return jax.shard_map(
        body,
        mesh=mesh,
        in_specs=(
            P("ep", "tp"), P("ep", "tp"), P("ep", "tp"), P("ep", "tp"), P("tp", None), P("ep", None), P(),
            P("ep", None), P("ep", None), P(None, "tp"), P(None, "tp"), P("tp", None),
            P("ep", None, "tp"), P("ep", None, "tp"), P("ep", "tp", None),
        ),
        out_specs=(P("ep", "tp"), P("ep", "tp")),
        check_vma=False,
    )
```

```python
import functools

import jax
import jax.numpy as jnp
from jax import lax
from jax.experimental import pallas as pl
from jax.experimental.pallas import tpu as pltpu
from jax.sharding import PartitionSpec as P

MESH = pl.DeviceIdType.MESH
BF = jnp.bfloat16
F32 = jnp.float32
NX, NZ, NY = 4, 8, 8
UP = 4
HELP = 3
SHIFT = UP + 1
BAND = 16
LOG2E = 1.4426950408889634
EPS_NORM = 1e-06
ROUTED_SCALE = 2.5
S = 512
H = 128
KB = 528
KVR = 1040
CAPP = 16
CAP = 12


def dot(a, b):
    return jnp.dot(a, b, preferred_element_type=F32)


def iota(shape, dim):
    return lax.broadcasted_iota(jnp.int32, shape, dim)


def attend(query, key, value, bias, first):
    half = S // 2
    logit = lax.dot_general(query, key, (((1,), (1,)), ((), ())), preferred_element_type=F32)
    logit = logit * (LOG2E / H**0.5) + bias
    soft = jnp.maximum(logit, jnp.log2(1.0 + jnp.exp2(jnp.minimum(logit, 100.0))))
    base = logit - soft
    if first is not None:
        visible = iota(soft.shape, 1) + first < iota(soft.shape, 0)
        soft = jnp.where(visible, soft, 0.0)
    soft = soft.astype(BF)
    later = jnp.where(iota((half, half), 0) > iota((half, half), 1), 1.0, 0.0).astype(BF)
    stay_hi = dot(soft[:, half:], later)
    sum_hi = stay_hi[:, 0:1] + soft[:, half : half + 1].astype(F32)
    stay_lo = dot(soft[:, :half], later) + sum_hi
    total = stay_lo[:, 0:1] + soft[:, 0:1].astype(F32)
    weight = jnp.exp2(base - jnp.concatenate([stay_lo, stay_hi], axis=1))
    if first is not None:
        weight = jnp.where(visible, weight, 0.0)
    return dot(weight.astype(BF), value), total


def kernel(
    q_in, k_in, v_in, bias_in, ow_in, mi_in, gain_in, ids_in, scores_in, sg_in, su_in, sd_in, eg_in, eu_in, ed_in,
    mixed, mix,
    qb, kvb, op, tcol, tr, ts, osend, orecv, hsend, hrecv, oacc, factor, heads,
    bias, gain, ids, scores, wgu, sgu, ed, sd, ow, mi, normed, gated,
    a1s, a1r, a2r, ag, b0, b1r, b2r, common,
    part_m, sib_m, ring_m, rsend_m, part_a, sib_a, ring_a, rsend_a,
    lsem, q_s, q_r, qh_s, qh_r, h_s, h_r, kv_s, kv_r, a1_s, a1_rs, a2_s, a2_rs, ag_s, ag_r, ags_s, ags_r,
    b1_s, b1_rs, b2_s, b2_rs, t_s, t_r, o_s, o_r,
    msib_s, msib_r, mring_s, mring_r, asib_s, asib_r, aring_s, aring_r,
):
    ep, tp = lax.axis_index("ep"), lax.axis_index("tp")
    z, x, y, c = ep // NX, ep % NX, tp // 2, tp % 2

    def at_x(d):
        return {"ep": z * NX + (x + d) % NX, "tp": tp}

    def at_z(d):
        return {"ep": ((z + d) % NZ) * NX + x, "tp": tp}

    def at_y(d):
        return {"ep": ep, "tp": ((y + d) % NY) * 2 + c}

    opposite = {"ep": (NZ - 1 - z) * NX + x, "tp": tp}

    helper, helped = z < HELP, z >= NZ - HELP
    sibling = {"ep": ep, "tp": y * 2 + (1 - c)}

    def send(src, dst, ssem, rsem, dev):
        return pltpu.make_async_remote_copy(
            src_ref=src, dst_ref=dst, send_sem=ssem, recv_sem=rsem, device_id=dev, device_id_type=MESH
        )

    local = [
        (q_in, qb.at[0, pl.ds(pl.multiple_of(x * S, S), S)]),
        (k_in, kvb.at[z, 0:S]),
        (v_in, kvb.at[z, KB:KVR]),
        (bias_in, bias),
        (mi_in, mi),
        (eg_in, wgu.at[:, 0:H]),
        (eu_in, wgu.at[:, H : 2 * H]),
        (sg_in, sgu.at[:, 0:H]),
        (su_in, sgu.at[:, H : 2 * H]),
        (ed_in, ed),
        (sd_in, sd),
        (ow_in, ow),
        (gain_in, gain),
        (ids_in, ids),
        (scores_in, scores),
    ]
    fetch = [pltpu.make_async_copy(a, b, lsem.at[i]) for i, (a, b) in enumerate(local)]

    barrier = pltpu.get_barrier_semaphore()
    partners = [at_x(d) for d in range(1, NX)] + [at_z(d) for d in range(1, NZ)]
    partners += [at_y(1), at_y(-1), sibling]
    for dev in partners:
        pl.semaphore_signal(barrier, inc=1, device_id=dev, device_id_type=MESH)
    for i in (4, 12, 13, 14, 3, 0, 1, 2, 5, 6, 7, 8, 9, 10, 11):
        fetch[i].start()

    pending = []

    def begin(copy, when=None):
        pending.append((when, copy))
        if when is None:
            copy.start()
        else:
            pl.when(when)(copy.start)

    halves = (slice(0, KB), slice(KB, KVR))

    def query_rows(i, which=0):
        return qb.at[which, pl.ds(pl.multiple_of(i * S, S), S)]

    def to_helper():
        return send(query_rows(x), query_rows(x, 1), qh_s.at[0], qh_r.at[0], opposite)

    def up(d, h):
        block = kvb.at[jnp.maximum(z - d + 1, 0), halves[h]]
        return send(block, block, kv_s.at[0, d - 1, h], kv_r.at[0, d - 1, h], at_z(1))

    def up_arrival(d, h):
        block = kvb.at[jnp.maximum(z - d, 0), halves[h]]
        return send(block, block, kv_s.at[0, d - 1, h], kv_r.at[0, d - 1, h], at_z(1))

    def down(d, h):
        block = kvb.at[jnp.minimum(z + d - 1, NZ - 1), halves[h]]
        return send(block, block, kv_s.at[1, d - 1, h], kv_r.at[1, d - 1, h], at_z(-1))

    def down_arrival(d, h):
        block = kvb.at[jnp.minimum(z + d, NZ - 1), halves[h]]
        return send(block, block, kv_s.at[1, d - 1, h], kv_r.at[1, d - 1, h], at_z(-1))

    def step(which, zi, place, first):
        rows = kvb[zi, S:KB, :].astype(F32) * LOG2E
        row = jnp.concatenate([rows[j : j + 1, :] for j in range(S // H)], axis=1)
        out, total = attend(qb[which], kvb[zi, 0:S, :], kvb[zi, KB:KVR, :], row, first)
        op[place] = out
        tcol[...] = jnp.where(iota((NX * S, H), 1) == place, total, tcol[...])

    def attention():
        fetch[0].wait()
        for d in range(1, NX):
            begin(send(query_rows(x), query_rows(x), q_s.at[d - 1], q_r.at[d - 1], at_x(d)))
        fetch[1].wait()
        sends_down = (z >= 1) & (z < HELP)
        begin(up(1, 0), z < NZ - 1)
        begin(down(1, 0), sends_down)
        fetch[2].wait()
        begin(up(1, 1), z < NZ - 1)
        begin(down(1, 1), sends_down)
        begin(to_helper(), helped)
        yield
        tcol[...] = jnp.zeros_like(tcol)
        for d in range(1, NX):
            src = query_rows((x - d + NX) % NX)
            send(src, src, q_s.at[d - 1], q_r.at[d - 1], at_x(d)).wait_recv()

        @pl.when(helper)
        def _():
            to_helper().wait_recv()

        for d in range(1, NX):
            begin(send(query_rows(x, 1), query_rows(x, 1), qh_s.at[d], qh_r.at[d], at_x(d)), helper)
        step(0, z, 0, x * S)
        yield
        for d in range(1, UP + 1):
            for h in range(2):

                @pl.when(z >= d)
                def _():
                    up_arrival(d, h).wait_recv()

                if d < UP:
                    begin(up(d + 1, h), (z >= d) & (z < NZ - 1))
                if d < HELP:

                    @pl.when(z < HELP - d)
                    def _():
                        down_arrival(d, h).wait_recv()

                    if d == 1:
                        begin(down(2, h), z == 1)
            if d == 2:

                @pl.when(helper)
                def _():
                    for i in range(1, NX):
                        src = query_rows((x - i + NX) % NX, 1)
                        send(src, src, qh_s.at[i], qh_r.at[i], at_x(i)).wait_recv()

            mine = z >= d
            older = jnp.maximum(d - z - 2, 0)
            zi = jnp.where(mine, z - d, older)

            @pl.when(mine | ((d >= z + 2) & (d <= HELP + 1)))
            def _():
                step(jnp.where(mine, 0, 1), zi, jnp.where(mine, d, SHIFT + older), None)

            yield
        for qi in range(NX):
            ts[qi] = tcol[qi * S : (qi + 1) * S].T[0:NZ, :]
        for d in range(1, NX):
            begin(send(ts, tr.at[x], t_s.at[d - 1], t_r.at[d - 1], at_x(d)))
        tr[x] = ts[...]
        yield
        for d in range(1, NX):
            src = tr.at[(x - d + NX) % NX]
            send(ts, src, t_s.at[d - 1], t_r.at[d - 1], at_x(d)).wait_recv()

        def scales(qi):
            sums = [tr[i, qi] for i in range(NX)]
            row = sums[0] + sums[1] + sums[2] + sums[3]
            within = sum(jnp.where(i > x, sums[i], 0.0) for i in range(1, NX))
            parts, nothing = [None] * NZ, jnp.zeros((1, S), F32)
            run = nothing
            for k in range(SHIFT):
                parts[k] = run
                run = run + row[k : k + 1, :]
            after = nothing
            for k in reversed(range(SHIFT, NZ)):
                parts[k] = after
                after = after + row[k : k + 1, :]
            carried = jnp.concatenate(parts, axis=0) + within
            return [jnp.exp2(-carried), jnp.exp2(-run), jnp.zeros((BAND - NZ - 1, S), F32)]

        order = (1, 2, 3, 0)
        bands = [part for d in order for part in scales((x + d) % NX)]
        bands.append(jnp.zeros((H - NX * BAND, S), F32))
        scale = jnp.concatenate(bands, axis=0).T

        def share(j, k, rows):
            return scale[:, j * BAND + k : j * BAND + k + 1] * op[k, rows, :]

        def combine(j, rows):
            @pl.when(z >= UP)
            def _():
                total = share(j, 0, rows)
                for k in range(1, UP + 1):
                    total = total + share(j, k, rows)
                oacc[...] = total

            @pl.when(z < UP)
            def _():
                oacc[...] = share(j, 0, rows)
                for k in range(1, UP):

                    @pl.when(k <= z)
                    def _():
                        oacc[...] += share(j, k, rows)

        def combine_helped(j, d, rows):
            @pl.when(helper)
            def _():
                oacc[...] = share(j, SHIFT, rows)
                for i in range(1, HELP):

                    @pl.when(i < HELP - z)
                    def _():
                        oacc[...] += share(j, SHIFT + i, rows)

                if d > 0:
                    hsend[d - 1] = oacc[...].astype(BF)
                else:
                    factor[...] = oacc[...]

            if d > 0:
                begin(help_out(d), helper)

        def help_out(d):
            return send(hsend.at[d - 1], hrecv.at[d - 1], h_s.at[d], h_r.at[d], at_x(d))

        def help_home():
            return send(hsend.at[NX - 1], hrecv.at[NX - 1], h_s.at[0], h_r.at[0], opposite)

        for j, d in enumerate(order):
            rows = pl.ds(pl.multiple_of(((x + d) % NX) * S, S), S)
            combine_helped(j, d, rows)
            combine(j, rows)
            if d > 0:
                osend[d - 1] = oacc[...].astype(BF)
                begin(send(osend.at[d - 1], orecv.at[d - 1], o_s.at[d - 1], o_r.at[d - 1], at_x(d)))
            else:
                heads[...] = oacc[...]

                @pl.when(helped)
                def _():
                    factor[...] = jnp.broadcast_to(scale[:, j * BAND + NZ : j * BAND + NZ + 1], (S, H))

        yield

        @pl.when(helper)
        def _():
            for d in range(1, NX):
                help_out(d).wait_recv()
            far = factor[...] + hrecv[0].astype(F32) + hrecv[1].astype(F32) + hrecv[2].astype(F32)
            hsend[NX - 1] = far.astype(BF)

        begin(help_home(), helper)
        for d in range(1, NX):
            send(osend.at[d - 1], orecv.at[d - 1], o_s.at[d - 1], o_r.at[d - 1], at_x(d)).wait_recv()
        heads[...] += orecv[0].astype(F32) + orecv[1].astype(F32) + orecv[2].astype(F32)

        @pl.when(helped)
        def _():
            help_home().wait_recv()
            heads[...] += factor[...] * hrecv[NX - 1].astype(F32)

        rounded = heads[...].astype(BF)
        fetch[11].wait()

        def fill(yi):
            both = dot(rounded, ow[:, pl.ds(pl.multiple_of(yi * 256, 256), 256)]).astype(BF)
            part_a[0, yi] = both[:, :H]
            part_a[1, yi] = both[:, H:]

        out = yield from reduce_scatter(
            fill, 2, part_a, sib_a, ring_a, rsend_a, asib_s, asib_r, aring_s, aring_r
        )
        mixed[...] = out.astype(BF)

    def reduce_scatter(fill, cuts, part, sib, ring, rsend, sib_s, sib_r, ring_s, ring_r):
        order = [4, -3, 3, -2, 2, -1, 1, 0]
        length = S // cuts
        spans = [slice(i * length, (i + 1) * length) for i in range(cuts)]

        def to_sibling(m):
            yi = (y + order[m] + NY) % NY
            return send(part.at[1 - c, yi], sib.at[m], sib_s.at[m], sib_r.at[m], sibling)

        for m in range(NY):
            fill((y + order[m] + NY) % NY)
            begin(to_sibling(m))
        yield

        def mine(m, span):
            yi = (y + order[m] + NY) % NY
            return part[c, yi, span].astype(F32) + sib[m, span].astype(F32)

        def hop(way, s, i):
            return send(
                rsend.at[way, s, spans[i]], ring.at[way, s, spans[i]],
                ring_s.at[way, s, i], ring_r.at[way, s, i], at_y(1 - 2 * way),
            )

        for s in range(4):
            for i in range(cuts):
                for way in range(2):
                    if way == 1 and s == 3:
                        continue
                    if i == 0:
                        to_sibling(2 * s + way).wait_recv()
                    value = mine(2 * s + way, spans[i])
                    if s > 0:
                        hop(way, s - 1, i).wait_recv()
                        value = value + ring[way, s - 1, spans[i]].astype(F32)
                    rsend[way, s, spans[i]] = value.astype(BF)
                    begin(hop(way, s, i))
            yield
        to_sibling(7).wait_recv()
        done = []
        for i in range(cuts):
            value = mine(7, spans[i])
            hop(1, 2, i).wait_recv()
            value = value + ring[1, 2, spans[i]].astype(F32)
            hop(0, 3, i).wait_recv()
            done.append(value + ring[0, 3, spans[i]].astype(F32))
        return jnp.concatenate(done, axis=0) if cuts > 1 else done[0]

    def spread(transposed):
        shape = (NZ * NX * CAPP, NZ * NX * CAP) if transposed else (NZ * NX * CAP, NZ * NX * CAPP)
        padded, packed = (iota(shape, 0), iota(shape, 1)) if transposed else (iota(shape, 1), iota(shape, 0))
        place = padded & (CAPP - 1)
        hit = ((padded >> 4) * CAP + place == packed) & (place < CAP)
        return jnp.where(hit, 1.0, 0.0).astype(BF)

    def experts():
        for i in (4, 12, 13, 14):
            fetch[i].wait()
        value = mi[...].astype(F32)
        mean = jnp.mean(value * value, axis=1, keepdims=True)
        normed[...] = (value * lax.rsqrt(mean + EPS_NORM) * gain[...]).astype(BF)
        facing = ((y + NY // 2) % NY) * 2 + c
        own = jnp.concatenate([normed[:, pl.ds(pl.multiple_of(i * H, H), H)] for i in (tp, facing)], axis=1)
        slots = NZ * NX * CAPP
        group = iota((slots, 128), 0) >> 4
        place = iota((slots, 128), 0) & (CAPP - 1)
        expert = (group & (NZ - 1)) * NX + (group >> 3)
        first, second = ids[0:1, :] == expert, ids[1:2, :] == expert
        named = first | second
        earlier = jnp.where(iota((128, 128), 0) < iota((128, 128), 1), 1.0, 0.0).astype(BF)
        count = dot(jnp.where(named, 1.0, 0.0).astype(BF), earlier)
        chosen = named & (count == place.astype(F32))
        scale = ROUTED_SCALE / (scores[0:1, :] + scores[1:2, :])
        gate = jnp.where(first, scores[0:1, :] * scale, 0.0) + jnp.where(second, scores[1:2, :] * scale, 0.0)
        gated[...] = jnp.where(chosen, gate, 0.0)
        out = dot(jnp.where(chosen, 1.0, 0.0).astype(BF), own).astype(BF)
        a1s[...] = out.reshape(NX, NZ, CAPP, 2 * H)
        fetch[3].wait()
        line = bias[...]
        line = [line[:, j * H : (j + 1) * H] for j in range(S // H)]
        kvb[z, S:KB, :] = jnp.concatenate(line + [jnp.zeros((KB - S - S // H, H), BF)], axis=0)
        pl.semaphore_wait(barrier, len(partners))

        def by_x(d):
            return send(a1s.at[(x + d) % NX], a1r.at[x], a1_s.at[d - 1], a1_rs.at[d - 1], at_x(d))

        for d in range(1, NX):
            begin(by_x(d))
        a1r[x] = a1s[x]
        yield
        for d in range(1, NX):
            send(a1s.at[x], a1r.at[(x - d + NX) % NX], a1_s.at[d - 1], a1_rs.at[d - 1], at_x(d)).wait_recv()
        for d in range(1, NZ):
            begin(send(a1r.at[:, (z + d) % NZ], a2r.at[z], a2_s.at[d - 1], a2_rs.at[d - 1], at_z(d)))
        a2r[z] = a1r[:, z]
        yield
        for d in range(1, NZ):
            send(a1r.at[:, z], a2r.at[(z - d + NZ) % NZ], a2_s.at[d - 1], a2_rs.at[d - 1], at_z(d)).wait_recv()
        packed = dot(spread(False), a2r[...].reshape(slots, 2 * H)).astype(BF)
        ag[tp] = packed[:, :H]
        ag[facing] = packed[:, H:]

        def slice_of(yi, core=c):
            return ag.at[((yi + NY) % NY) * 2 + core]

        def along(way, n, yi):
            return send(slice_of(yi), slice_of(yi), ag_s.at[way, n], ag_r.at[way, n], at_y(1 - 2 * way))

        def across(m, yi, core):
            return send(slice_of(yi, core), slice_of(yi, core), ags_s.at[m], ags_r.at[m], sibling)

        for n in range(2):
            for way in range(2):
                begin(along(way, n, y + n * NY // 2))
        begin(across(0, y, c))
        begin(across(1, y + NY // 2, c))
        yield
        for way in range(2):
            near = y - (1 - 2 * way)
            along(way, 0, near).wait_recv()
            begin(along(way, 2, near))
            begin(across(2 + way, near, c))
        yield
        for n in range(1, 3):
            for way in range(2):
                sign = 1 - 2 * way
                came = y - sign + NY // 2 if n == 1 else y - 2 * sign
                along(way, n, came).wait_recv()
                begin(across(2 + 2 * n + way, came, c))
        yield
        across(0, y, 1 - c).wait_recv()
        across(1, y + NY // 2, 1 - c).wait_recv()
        for way in range(2):
            sign = 1 - 2 * way
            across(2 + way, y - sign, 1 - c).wait_recv()
            across(4 + way, y - sign + NY // 2, 1 - c).wait_recv()
            across(6 + way, y - 2 * sign, 1 - c).wait_recv()
        for i in (5, 6, 7, 8, 9, 10):
            fetch[i].wait()
        acc = jnp.zeros((NZ * NX * CAP, 2 * H), F32)
        acc_s = jnp.zeros((128, 2 * H), F32)
        for j in range(NY):
            wide = jnp.concatenate([ag[2 * j], ag[2 * j + 1]], axis=1)
            acc = acc + dot(wide, wgu[j * 256 : (j + 1) * 256, :])
            acc_s = acc_s + dot(normed[:, j * 256 : (j + 1) * 256], sgu[j * 256 : (j + 1) * 256, :])

        def swiglu(a):
            g, u = a[:, :H], a[:, H:]
            return (g / (1.0 + jnp.exp(-g)) * u).astype(BF)

        hidden, hidden_s = swiglu(acc), swiglu(acc_s)
        rows = NZ * NX * CAP

        def fill(yi):
            cols = pl.ds(pl.multiple_of(yi * 256, 256), 256)
            both = dot(hidden, ed[:, cols]).astype(BF)
            part_m[0, yi, 0:rows] = both[:, :H]
            part_m[1, yi, 0:rows] = both[:, H:]
            both = dot(hidden_s, sd[:, cols]).astype(BF)
            part_m[0, yi, rows:S] = both[:, :H]
            part_m[1, yi, rows:S] = both[:, H:]

        out = yield from reduce_scatter(
            fill, 2, part_m, sib_m, ring_m, rsend_m, msib_s, msib_r, mring_s, mring_r
        )
        common[...] = out[rows:S, :]
        b0[...] = dot(spread(True), out[0:rows, :].astype(BF)).astype(BF).reshape(NZ, NX, CAPP, H)
        for d in range(1, NZ):
            begin(send(b0.at[(z + d) % NZ], b1r.at[z], b1_s.at[d - 1], b1_rs.at[d - 1], at_z(d)))
        b1r[z] = b0[z]
        yield
        for d in range(1, NZ):
            send(b0.at[z], b1r.at[(z - d + NZ) % NZ], b1_s.at[d - 1], b1_rs.at[d - 1], at_z(d)).wait_recv()
        for d in range(1, NX):
            begin(send(b1r.at[:, (x + d) % NX], b2r.at[x], b2_s.at[d - 1], b2_rs.at[d - 1], at_x(d)))
        b2r[x] = b1r[:, x]
        yield
        for d in range(1, NX):
            send(b1r.at[:, x], b2r.at[(x - d + NX) % NX], b2_s.at[d - 1], b2_rs.at[d - 1], at_x(d)).wait_recv()
        gates = gated[...].T
        high = gates.astype(BF)
        low = (gates - high.astype(F32)).astype(BF)
        got = b2r[...].reshape(slots, H)
        mix[...] = (common[...] + dot(high, got) + dot(low, got)).astype(BF)

    attn, moe = attention(), experts()
    for turn in "mamamamamamamaamamamamaamam":
        next(attn if turn == "a" else moe, None)

    for when, copy in pending:
        if when is None:
            copy.wait_send()
        else:
            pl.when(when)(copy.wait_send)


def body(
    queries, keys, values, key_bias, out_weight, moe_input, moe_gain, route_ids, route_scores,
    shared_gate, shared_up, shared_down, expert_gate, expert_up, expert_down,
):
    hbm, vmem = pl.BlockSpec(memory_space=pl.ANY), pl.BlockSpec(memory_space=pltpu.VMEM)
    dma = pltpu.SemaphoreType.DMA
    V = pltpu.VMEM
    slots = (NZ, NX, CAPP, H)
    rs = [V((2, NY, S, H), BF), V((NY, S, H), BF), V((2, 4, S, H), BF), V((2, 4, S, H), BF)]
    sems = [dma((15,)), dma((3,)), dma((3,)), dma((4,)), dma((4,)), dma((4,)), dma((4,)), dma((2, 4, 2)), dma((2, 4, 2)), dma((3,)), dma((3,)), dma((7,)), dma((7,))]
    sems += [dma((2, 4)), dma((2, 4)), dma((8,)), dma((8,))]
    sems += [dma((7,)), dma((7,)), dma((3,)), dma((3,)), dma((3,)), dma((3,)), dma((3,)), dma((3,))]
    sems += [dma((8,)), dma((8,)), dma((2, 4, 2)), dma((2, 4, 2))] * 2
    return pl.pallas_call(
        kernel,
        out_shape=(jax.ShapeDtypeStruct((S, H), BF), jax.ShapeDtypeStruct((128, H), BF)),
        in_specs=[hbm] * 15,
        out_specs=(vmem, vmem),
        scratch_shapes=[
            V((2, NX * S, H), BF), V((NZ, KVR, H), BF), V((NZ, NX * S, H), F32), V((NX * S, H), F32),
            V((NX, NX, NZ, S), F32), V((NX, NZ, S), F32), V((NX - 1, S, H), BF), V((NX - 1, S, H), BF),
            V((NX, S, H), BF), V((NX, S, H), BF), V((S, H), F32), V((S, H), F32), V((S, H), F32),
            V((1, S), BF), V((1, 2048), F32), V((2, 128), jnp.int32), V((2, 128), F32),
            V((2048, 2 * H), BF), V((2048, 2 * H), BF), V((H, 2048), BF), V((H, 2048), BF), V((H, 2048), BF),
            V((128, 2048), BF), V((128, 2048), BF), V((512, 128), F32),
            V((NX, NZ, CAPP, 2 * H), BF), V((NX, NZ, CAPP, 2 * H), BF), V((NZ, NX, CAPP, 2 * H), BF), V((16, NZ * NX * CAP, H), BF),
            V(slots, BF), V(slots, BF), V((NX, NZ, CAPP, H), BF), V((128, H), F32),
            *rs, *rs, *sems,
        ],
        compiler_params=pltpu.CompilerParams(
            collective_id=0, has_side_effects=True, vmem_limit_bytes=60 * 2**20
        ),
        name="fused",
    )(
        queries, keys, values, key_bias.T, out_weight, moe_input, moe_gain.reshape(1, -1), route_ids.T, route_scores.T,
        shared_gate, shared_up, shared_down,
        expert_gate.reshape(2048, H), expert_up.reshape(2048, H), expert_down.reshape(H, 2048),
    )


def solution(mesh):
    return jax.shard_map(
        body,
        mesh=mesh,
        in_specs=(
            P("ep", "tp"), P("ep", "tp"), P("ep", "tp"), P("ep", "tp"), P("tp", None), P("ep", None), P(),
            P("ep", None), P("ep", None), P(None, "tp"), P(None, "tp"), P("tp", None),
            P("ep", None, "tp"), P("ep", None, "tp"), P("ep", "tp", None),
        ),
        out_specs=(P("ep", "tp"), P("ep", "tp")),
        check_vma=False,
    )
```

```python
import functools

import jax
import jax.numpy as jnp
from jax import lax
from jax.experimental import pallas as pl
from jax.experimental.pallas import tpu as pltpu
from jax.sharding import PartitionSpec as P

MESH = pl.DeviceIdType.MESH
BF = jnp.bfloat16
F32 = jnp.float32
NX, NZ, NY = 4, 8, 8
UP = 4
HELP = 3
SHIFT = UP + 1
BAND = 16
LOG2E = 1.4426950408889634
EPS_NORM = 1e-06
ROUTED_SCALE = 2.5
S = 512
H = 128
KB = 528
KVR = 1040
CAPP = 16
CAP = 12


def dot(a, b):
    return jnp.dot(a, b, preferred_element_type=F32)


def iota(shape, dim):
    return lax.broadcasted_iota(jnp.int32, shape, dim)


def attend(query, key, value, bias, first):
    half = S // 2
    logit = lax.dot_general(query, key, (((1,), (1,)), ((), ())), preferred_element_type=F32)
    logit = logit * (LOG2E / H**0.5) + bias
    soft = jnp.maximum(logit, jnp.log2(1.0 + jnp.exp2(jnp.minimum(logit, 100.0))))
    base = logit - soft
    if first is not None:
        visible = iota(soft.shape, 1) + first < iota(soft.shape, 0)
        soft = jnp.where(visible, soft, 0.0)
    soft = soft.astype(BF)
    later = jnp.where(iota((half, half), 0) > iota((half, half), 1), 1.0, 0.0).astype(BF)
    stay_hi = dot(soft[:, half:], later)
    sum_hi = stay_hi[:, 0:1] + soft[:, half : half + 1].astype(F32)
    stay_lo = dot(soft[:, :half], later) + sum_hi
    total = stay_lo[:, 0:1] + soft[:, 0:1].astype(F32)
    weight = jnp.exp2(base - jnp.concatenate([stay_lo, stay_hi], axis=1))
    if first is not None:
        weight = jnp.where(visible, weight, 0.0)
    return dot(weight.astype(BF), value), total


def kernel(
    q_in, k_in, v_in, bias_in, ow_in, mi_in, gain_in, ids_in, scores_in, sg_in, su_in, sd_in, eg_in, eu_in, ed_in,
    mixed, mix,
    qb, kvb, op, tcol, tr, ts, tr2, ts2, osend, orecv, hsend, hrecv, oacc, factor, heads,
    bias, gain, ids, scores, wgu, sgu, ed, sd, ow, mi, normed, gated,
    a1s, a1r, a2r, ag, b0, b1r, b2r, common,
    part_m, sib_m, ring_m, rsend_m, part_a, sib_a, ring_a, rsend_a,
    lsem, q_s, q_r, qh_s, qh_r, h_s, h_r, kv_s, kv_r, a1_s, a1_rs, a2_s, a2_rs, ag_s, ag_r, ags_s, ags_r,
    b1_s, b1_rs, b2_s, b2_rs, t_s, t_r, t2_s, t2_r, o_s, o_r,
    msib_s, msib_r, mring_s, mring_r, asib_s, asib_r, aring_s, aring_r,
):
    ep, tp = lax.axis_index("ep"), lax.axis_index("tp")
    z, x, y, c = ep // NX, ep % NX, tp // 2, tp % 2

    def at_x(d):
        return {"ep": z * NX + (x + d) % NX, "tp": tp}

    def at_z(d):
        return {"ep": ((z + d) % NZ) * NX + x, "tp": tp}

    def at_y(d):
        return {"ep": ep, "tp": ((y + d) % NY) * 2 + c}

    opposite = {"ep": (NZ - 1 - z) * NX + x, "tp": tp}

    helper, helped = z < HELP, z >= NZ - HELP
    sibling = {"ep": ep, "tp": y * 2 + (1 - c)}

    def send(src, dst, ssem, rsem, dev):
        return pltpu.make_async_remote_copy(
            src_ref=src, dst_ref=dst, send_sem=ssem, recv_sem=rsem, device_id=dev, device_id_type=MESH
        )

    local = [
        (q_in, qb.at[0, pl.ds(pl.multiple_of(x * S, S), S)]),
        (k_in, kvb.at[z, 0:S]),
        (v_in, kvb.at[z, KB:KVR]),
        (bias_in, bias),
        (mi_in, mi),
        (eg_in, wgu.at[:, 0:H]),
        (eu_in, wgu.at[:, H : 2 * H]),
        (sg_in, sgu.at[:, 0:H]),
        (su_in, sgu.at[:, H : 2 * H]),
        (ed_in, ed),
        (sd_in, sd),
        (ow_in, ow),
        (gain_in, gain),
        (ids_in, ids),
        (scores_in, scores),
    ]
    fetch = [pltpu.make_async_copy(a, b, lsem.at[i]) for i, (a, b) in enumerate(local)]

    barrier = pltpu.get_barrier_semaphore()
    partners = [at_x(d) for d in range(1, NX)] + [at_z(d) for d in range(1, NZ)]
    partners += [at_y(1), at_y(-1), sibling]
    for dev in partners:
        pl.semaphore_signal(barrier, inc=1, device_id=dev, device_id_type=MESH)
    for i in (4, 12, 13, 14, 3, 0, 1, 2, 5, 6, 7, 8, 9, 10, 11):
        fetch[i].start()

    pending = []

    def begin(copy, when=None):
        pending.append((when, copy))
        if when is None:
            copy.start()
        else:
            pl.when(when)(copy.start)

    halves = (slice(0, KB), slice(KB, KVR))

    def query_rows(i, which=0):
        return qb.at[which, pl.ds(pl.multiple_of(i * S, S), S)]

    def to_helper():
        return send(query_rows(x), query_rows(x, 1), qh_s.at[0], qh_r.at[0], opposite)

    def up(d, h):
        block = kvb.at[jnp.maximum(z - d + 1, 0), halves[h]]
        return send(block, block, kv_s.at[0, d - 1, h], kv_r.at[0, d - 1, h], at_z(1))

    def up_arrival(d, h):
        block = kvb.at[jnp.maximum(z - d, 0), halves[h]]
        return send(block, block, kv_s.at[0, d - 1, h], kv_r.at[0, d - 1, h], at_z(1))

    def down(d, h):
        block = kvb.at[jnp.minimum(z + d - 1, NZ - 1), halves[h]]
        return send(block, block, kv_s.at[1, d - 1, h], kv_r.at[1, d - 1, h], at_z(-1))

    def down_arrival(d, h):
        block = kvb.at[jnp.minimum(z + d, NZ - 1), halves[h]]
        return send(block, block, kv_s.at[1, d - 1, h], kv_r.at[1, d - 1, h], at_z(-1))

    def step(which, zi, place, first):
        rows = kvb[zi, S:KB, :].astype(F32) * LOG2E
        row = jnp.concatenate([rows[j : j + 1, :] for j in range(S // H)], axis=1)
        out, total = attend(qb[which], kvb[zi, 0:S, :], kvb[zi, KB:KVR, :], row, first)
        op[place] = out
        tcol[...] = jnp.where(iota((NX * S, H), 1) == place, total, tcol[...])

    def attention():
        fetch[0].wait()
        for d in range(1, NX):
            begin(send(query_rows(x), query_rows(x), q_s.at[d - 1], q_r.at[d - 1], at_x(d)))
        fetch[1].wait()
        sends_down = (z >= 1) & (z < HELP)
        begin(up(1, 0), z < NZ - 1)
        begin(down(1, 0), sends_down)
        fetch[2].wait()
        begin(up(1, 1), z < NZ - 1)
        begin(down(1, 1), sends_down)
        begin(to_helper(), helped)
        yield
        tcol[...] = jnp.zeros_like(tcol)
        for d in range(1, NX):
            src = query_rows((x - d + NX) % NX)
            send(src, src, q_s.at[d - 1], q_r.at[d - 1], at_x(d)).wait_recv()

        @pl.when(helper)
        def _():
            to_helper().wait_recv()

        for d in range(1, NX):
            begin(send(query_rows(x, 1), query_rows(x, 1), qh_s.at[d], qh_r.at[d], at_x(d)), helper)
        step(0, z, 0, x * S)
        yield
        def sums_of(qi):
            return tcol[qi * S : (qi + 1) * S].T[0:NZ, :]

        for d in range(1, UP + 1):
            for h in range(2):

                @pl.when(z >= d)
                def _():
                    up_arrival(d, h).wait_recv()

                if d < UP:
                    begin(up(d + 1, h), (z >= d) & (z < NZ - 1))
                if d == 1 or d == HELP:
                    hops = 1 if d == 1 else HELP - 1

                    @pl.when(z < HELP - hops)
                    def _():
                        down_arrival(hops, h).wait_recv()

                    if d == 1:
                        begin(down(2, h), z == 1)
            if d <= HELP:

                @pl.when(z == d - 1)
                def _():
                    for i in range(1, NX):
                        src = query_rows((x - i + NX) % NX, 1)
                        send(src, src, qh_s.at[i], qh_r.at[i], at_x(i)).wait_recv()

            mine = z >= d
            older = jnp.maximum(d - z - 1, 0)
            zi = jnp.where(mine, z - d, older)

            @pl.when(mine | (d <= HELP))
            def _():
                step(jnp.where(mine, 0, 1), zi, jnp.where(mine, d, SHIFT + older), None)

            if d == UP - 1:
                for qi in range(NX):
                    ts[qi] = sums_of(qi)
                for i in range(1, NX):
                    begin(send(ts, tr.at[x], t_s.at[i - 1], t_r.at[i - 1], at_x(i)))
                tr[x] = ts[...]
            yield
        newest = iota((NZ, S), 0) == UP
        for qi in range(NX):
            ts2[qi] = jnp.sum(jnp.where(newest, sums_of(qi), 0.0), axis=0, keepdims=True)
        for d in range(1, NX):
            begin(send(ts2, tr2.at[x], t2_s.at[d - 1], t2_r.at[d - 1], at_x(d)))
        tr2[x] = ts2[...]
        yield
        for d in range(1, NX):
            src, src2 = tr.at[(x - d + NX) % NX], tr2.at[(x - d + NX) % NX]
            send(ts, src, t_s.at[d - 1], t_r.at[d - 1], at_x(d)).wait_recv()
            send(ts2, src2, t2_s.at[d - 1], t2_r.at[d - 1], at_x(d)).wait_recv()

        def scales(qi):
            sums = [tr[i, qi] + jnp.where(newest, tr2[i, qi], 0.0) for i in range(NX)]
            row = sums[0] + sums[1] + sums[2] + sums[3]
            within = sum(jnp.where(i > x, sums[i], 0.0) for i in range(1, NX))
            parts, nothing = [None] * NZ, jnp.zeros((1, S), F32)
            run = nothing
            for k in range(SHIFT):
                parts[k] = run
                run = run + row[k : k + 1, :]
            after = nothing
            for k in reversed(range(SHIFT, NZ)):
                parts[k] = after
                after = after + row[k : k + 1, :]
            carried = jnp.concatenate(parts, axis=0) + within
            return [jnp.exp2(-carried), jnp.exp2(-run), jnp.zeros((BAND - NZ - 1, S), F32)]

        order = (1, 2, 3, 0)
        bands = [part for d in order for part in scales((x + d) % NX)]
        bands.append(jnp.zeros((H - NX * BAND, S), F32))
        scale = jnp.concatenate(bands, axis=0).T

        def share(j, k, rows):
            return scale[:, j * BAND + k : j * BAND + k + 1] * op[k, rows, :]

        def combine(j, rows):
            @pl.when(z >= UP)
            def _():
                total = share(j, 0, rows)
                for k in range(1, UP + 1):
                    total = total + share(j, k, rows)
                oacc[...] = total

            @pl.when(z < UP)
            def _():
                oacc[...] = share(j, 0, rows)
                for k in range(1, UP):

                    @pl.when(k <= z)
                    def _():
                        oacc[...] += share(j, k, rows)

        def combine_helped(j, d, rows):
            @pl.when(helper)
            def _():
                oacc[...] = share(j, SHIFT, rows)
                for i in range(1, HELP):

                    @pl.when(i < HELP - z)
                    def _():
                        oacc[...] += share(j, SHIFT + i, rows)

                if d > 0:
                    hsend[d - 1] = oacc[...].astype(BF)
                else:
                    factor[...] = oacc[...]

            if d > 0:
                begin(help_out(d), helper)

        def help_out(d):
            return send(hsend.at[d - 1], hrecv.at[d - 1], h_s.at[d], h_r.at[d], at_x(d))

        def help_home():
            return send(hsend.at[NX - 1], hrecv.at[NX - 1], h_s.at[0], h_r.at[0], opposite)

        for j, d in enumerate(order):
            combine_helped(j, d, pl.ds(pl.multiple_of(((x + d) % NX) * S, S), S))
        for j, d in enumerate(order):
            combine(j, pl.ds(pl.multiple_of(((x + d) % NX) * S, S), S))
            if d > 0:
                osend[d - 1] = oacc[...].astype(BF)
                begin(send(osend.at[d - 1], orecv.at[d - 1], o_s.at[d - 1], o_r.at[d - 1], at_x(d)))
            else:
                heads[...] = oacc[...]

                @pl.when(helped)
                def _():
                    factor[...] = jnp.broadcast_to(scale[:, j * BAND + NZ : j * BAND + NZ + 1], (S, H))

        yield

        @pl.when(helper)
        def _():
            for d in range(1, NX):
                help_out(d).wait_recv()
            far = factor[...] + hrecv[0].astype(F32) + hrecv[1].astype(F32) + hrecv[2].astype(F32)
            hsend[NX - 1] = far.astype(BF)

        begin(help_home(), helper)
        yield
        for d in range(1, NX):
            send(osend.at[d - 1], orecv.at[d - 1], o_s.at[d - 1], o_r.at[d - 1], at_x(d)).wait_recv()
        heads[...] += orecv[0].astype(F32) + orecv[1].astype(F32) + orecv[2].astype(F32)

        @pl.when(helped)
        def _():
            help_home().wait_recv()
            heads[...] += factor[...] * hrecv[NX - 1].astype(F32)

        rounded = heads[...].astype(BF)
        fetch[11].wait()

        def fill(yi):
            both = dot(rounded, ow[:, pl.ds(pl.multiple_of(yi * 256, 256), 256)]).astype(BF)
            part_a[0, yi] = both[:, :H]
            part_a[1, yi] = both[:, H:]

        out = yield from reduce_scatter(
            fill, 4, part_a, sib_a, ring_a, rsend_a, asib_s, asib_r, aring_s, aring_r
        )
        mixed[...] = out.astype(BF)

    def reduce_scatter(fill, cuts, part, sib, ring, rsend, sib_s, sib_r, ring_s, ring_r):
        order = [4, -3, 3, -2, 2, -1, 1, 0]
        length = S // cuts
        spans = [slice(i * length, (i + 1) * length) for i in range(cuts)]

        def to_sibling(m):
            yi = (y + order[m] + NY) % NY
            return send(part.at[1 - c, yi], sib.at[m], sib_s.at[m], sib_r.at[m], sibling)

        for m in range(NY):
            fill((y + order[m] + NY) % NY)
            begin(to_sibling(m))
        yield

        def mine(m, span):
            yi = (y + order[m] + NY) % NY
            return part[c, yi, span].astype(F32) + sib[m, span].astype(F32)

        def hop(way, s, i):
            return send(
                rsend.at[way, s, spans[i]], ring.at[way, s, spans[i]],
                ring_s.at[way, s, i], ring_r.at[way, s, i], at_y(1 - 2 * way),
            )

        for s in range(4):
            for i in range(cuts):
                for way in range(2):
                    if way == 1 and s == 3:
                        continue
                    if i == 0:
                        to_sibling(2 * s + way).wait_recv()
                    value = mine(2 * s + way, spans[i])
                    if s > 0:
                        hop(way, s - 1, i).wait_recv()
                        value = value + ring[way, s - 1, spans[i]].astype(F32)
                    rsend[way, s, spans[i]] = value.astype(BF)
                    begin(hop(way, s, i))
            yield
        to_sibling(7).wait_recv()
        done = []
        for i in range(cuts):
            value = mine(7, spans[i])
            hop(1, 2, i).wait_recv()
            value = value + ring[1, 2, spans[i]].astype(F32)
            hop(0, 3, i).wait_recv()
            done.append(value + ring[0, 3, spans[i]].astype(F32))
        return jnp.concatenate(done, axis=0) if cuts > 1 else done[0]

    def spread(transposed):
        shape = (NZ * NX * CAPP, NZ * NX * CAP) if transposed else (NZ * NX * CAP, NZ * NX * CAPP)
        padded, packed = (iota(shape, 0), iota(shape, 1)) if transposed else (iota(shape, 1), iota(shape, 0))
        place = padded & (CAPP - 1)
        hit = ((padded >> 4) * CAP + place == packed) & (place < CAP)
        return jnp.where(hit, 1.0, 0.0).astype(BF)

    def experts():
        for i in (4, 12, 13, 14):
            fetch[i].wait()
        value = mi[...].astype(F32)
        mean = jnp.mean(value * value, axis=1, keepdims=True)
        normed[...] = (value * lax.rsqrt(mean + EPS_NORM) * gain[...]).astype(BF)
        facing = ((y + NY // 2) % NY) * 2 + c
        own = jnp.concatenate([normed[:, pl.ds(pl.multiple_of(i * H, H), H)] for i in (tp, facing)], axis=1)
        slots = NZ * NX * CAPP
        group = iota((slots, 128), 0) >> 4
        place = iota((slots, 128), 0) & (CAPP - 1)
        expert = (group & (NZ - 1)) * NX + (group >> 3)
        first, second = ids[0:1, :] == expert, ids[1:2, :] == expert
        named = first | second
        earlier = jnp.where(iota((128, 128), 0) < iota((128, 128), 1), 1.0, 0.0).astype(BF)
        count = dot(jnp.where(named, 1.0, 0.0).astype(BF), earlier)
        chosen = named & (count == place.astype(F32))
        scale = ROUTED_SCALE / (scores[0:1, :] + scores[1:2, :])
        gate = jnp.where(first, scores[0:1, :] * scale, 0.0) + jnp.where(second, scores[1:2, :] * scale, 0.0)
        gated[...] = jnp.where(chosen, gate, 0.0)
        out = dot(jnp.where(chosen, 1.0, 0.0).astype(BF), own).astype(BF)
        a1s[...] = out.reshape(NX, NZ, CAPP, 2 * H)
        fetch[3].wait()
        line = bias[...]
        line = [line[:, j * H : (j + 1) * H] for j in range(S // H)]
        kvb[z, S:KB, :] = jnp.concatenate(line + [jnp.zeros((KB - S - S // H, H), BF)], axis=0)
        pl.semaphore_wait(barrier, len(partners))

        def by_x(d):
            return send(a1s.at[(x + d) % NX], a1r.at[x], a1_s.at[d - 1], a1_rs.at[d - 1], at_x(d))

        for d in range(1, NX):
            begin(by_x(d))
        a1r[x] = a1s[x]
        yield
        for d in range(1, NX):
            send(a1s.at[x], a1r.at[(x - d + NX) % NX], a1_s.at[d - 1], a1_rs.at[d - 1], at_x(d)).wait_recv()
        for d in range(1, NZ):
            begin(send(a1r.at[:, (z + d) % NZ], a2r.at[z], a2_s.at[d - 1], a2_rs.at[d - 1], at_z(d)))
        a2r[z] = a1r[:, z]
        yield
        for d in range(1, NZ):
            send(a1r.at[:, z], a2r.at[(z - d + NZ) % NZ], a2_s.at[d - 1], a2_rs.at[d - 1], at_z(d)).wait_recv()
        packed = dot(spread(False), a2r[...].reshape(slots, 2 * H)).astype(BF)
        ag[tp] = packed[:, :H]
        ag[facing] = packed[:, H:]

        def slice_of(yi, core=c):
            return ag.at[((yi + NY) % NY) * 2 + core]

        def along(way, n, yi):
            return send(slice_of(yi), slice_of(yi), ag_s.at[way, n], ag_r.at[way, n], at_y(1 - 2 * way))

        def across(m, yi, core):
            return send(slice_of(yi, core), slice_of(yi, core), ags_s.at[m], ags_r.at[m], sibling)

        for n in range(2):
            for way in range(2):
                begin(along(way, n, y + n * NY // 2))
        begin(across(0, y, c))
        begin(across(1, y + NY // 2, c))
        yield
        for way in range(2):
            near = y - (1 - 2 * way)
            along(way, 0, near).wait_recv()
            begin(along(way, 2, near))
            begin(across(2 + way, near, c))
        yield
        for n in range(1, 3):
            for way in range(2):
                sign = 1 - 2 * way
                came = y - sign + NY // 2 if n == 1 else y - 2 * sign
                along(way, n, came).wait_recv()
                begin(across(2 + 2 * n + way, came, c))
        yield
        across(0, y, 1 - c).wait_recv()
        across(1, y + NY // 2, 1 - c).wait_recv()
        for way in range(2):
            sign = 1 - 2 * way
            across(2 + way, y - sign, 1 - c).wait_recv()
            across(4 + way, y - sign + NY // 2, 1 - c).wait_recv()
            across(6 + way, y - 2 * sign, 1 - c).wait_recv()
        for i in (5, 6, 7, 8, 9, 10):
            fetch[i].wait()
        acc = jnp.zeros((NZ * NX * CAP, 2 * H), F32)
        acc_s = jnp.zeros((128, 2 * H), F32)
        for j in range(NY):
            wide = jnp.concatenate([ag[2 * j], ag[2 * j + 1]], axis=1)
            acc = acc + dot(wide, wgu[j * 256 : (j + 1) * 256, :])
            acc_s = acc_s + dot(normed[:, j * 256 : (j + 1) * 256], sgu[j * 256 : (j + 1) * 256, :])

        def swiglu(a):
            g, u = a[:, :H], a[:, H:]
            return (g / (1.0 + jnp.exp(-g)) * u).astype(BF)

        hidden, hidden_s = swiglu(acc), swiglu(acc_s)
        rows = NZ * NX * CAP

        def fill(yi):
            cols = pl.ds(pl.multiple_of(yi * 256, 256), 256)
            both = dot(hidden, ed[:, cols]).astype(BF)
            part_m[0, yi, 0:rows] = both[:, :H]
            part_m[1, yi, 0:rows] = both[:, H:]
            both = dot(hidden_s, sd[:, cols]).astype(BF)
            part_m[0, yi, rows:S] = both[:, :H]
            part_m[1, yi, rows:S] = both[:, H:]

        out = yield from reduce_scatter(
            fill, 2, part_m, sib_m, ring_m, rsend_m, msib_s, msib_r, mring_s, mring_r
        )
        common[...] = out[rows:S, :]
        b0[...] = dot(spread(True), out[0:rows, :].astype(BF)).astype(BF).reshape(NZ, NX, CAPP, H)
        for d in range(1, NZ):
            begin(send(b0.at[(z + d) % NZ], b1r.at[z], b1_s.at[d - 1], b1_rs.at[d - 1], at_z(d)))
        b1r[z] = b0[z]
        yield
        for d in range(1, NZ):
            send(b0.at[z], b1r.at[(z - d + NZ) % NZ], b1_s.at[d - 1], b1_rs.at[d - 1], at_z(d)).wait_recv()
        for d in range(1, NX):
            begin(send(b1r.at[:, (x + d) % NX], b2r.at[x], b2_s.at[d - 1], b2_rs.at[d - 1], at_x(d)))
        b2r[x] = b1r[:, x]
        yield
        for d in range(1, NX):
            send(b1r.at[:, x], b2r.at[(x - d + NX) % NX], b2_s.at[d - 1], b2_rs.at[d - 1], at_x(d)).wait_recv()
        gates = gated[...].T
        high = gates.astype(BF)
        low = (gates - high.astype(F32)).astype(BF)
        got = b2r[...].reshape(slots, H)
        mix[...] = (common[...] + dot(high, got) + dot(low, got)).astype(BF)

    attn, moe = attention(), experts()
    for turn in "mamamaamammamaamamamamaamama":
        next(attn if turn == "a" else moe, None)

    for when, copy in pending:
        if when is None:
            copy.wait_send()
        else:
            pl.when(when)(copy.wait_send)


def body(
    queries, keys, values, key_bias, out_weight, moe_input, moe_gain, route_ids, route_scores,
    shared_gate, shared_up, shared_down, expert_gate, expert_up, expert_down,
):
    hbm, vmem = pl.BlockSpec(memory_space=pl.ANY), pl.BlockSpec(memory_space=pltpu.VMEM)
    dma = pltpu.SemaphoreType.DMA
    V = pltpu.VMEM
    slots = (NZ, NX, CAPP, H)
    rs = [V((2, NY, S, H), BF), V((NY, S, H), BF), V((2, 4, S, H), BF), V((2, 4, S, H), BF)]
    sems = [dma((15,)), dma((3,)), dma((3,)), dma((4,)), dma((4,)), dma((4,)), dma((4,)), dma((2, 4, 2)), dma((2, 4, 2)), dma((3,)), dma((3,)), dma((7,)), dma((7,))]
    sems += [dma((2, 4)), dma((2, 4)), dma((8,)), dma((8,))]
    sems += [dma((7,)), dma((7,)), dma((3,)), dma((3,)), dma((3,)), dma((3,)), dma((3,)), dma((3,)), dma((3,)), dma((3,))]
    sems += [dma((8,)), dma((8,)), dma((2, 4, 4)), dma((2, 4, 4))] * 2
    return pl.pallas_call(
        kernel,
        out_shape=(jax.ShapeDtypeStruct((S, H), BF), jax.ShapeDtypeStruct((128, H), BF)),
        in_specs=[hbm] * 15,
        out_specs=(vmem, vmem),
        scratch_shapes=[
            V((2, NX * S, H), BF), V((NZ, KVR, H), BF), V((NZ, NX * S, H), F32), V((NX * S, H), F32),
            V((NX, NX, NZ, S), F32), V((NX, NZ, S), F32), V((NX, NX, 1, S), F32), V((NX, 1, S), F32),
            V((NX - 1, S, H), BF), V((NX - 1, S, H), BF),
            V((NX, S, H), BF), V((NX, S, H), BF), V((S, H), F32), V((S, H), F32), V((S, H), F32),
            V((1, S), BF), V((1, 2048), F32), V((2, 128), jnp.int32), V((2, 128), F32),
            V((2048, 2 * H), BF), V((2048, 2 * H), BF), V((H, 2048), BF), V((H, 2048), BF), V((H, 2048), BF),
            V((128, 2048), BF), V((128, 2048), BF), V((512, 128), F32),
            V((NX, NZ, CAPP, 2 * H), BF), V((NX, NZ, CAPP, 2 * H), BF), V((NZ, NX, CAPP, 2 * H), BF), V((16, NZ * NX * CAP, H), BF),
            V(slots, BF), V(slots, BF), V((NX, NZ, CAPP, H), BF), V((128, H), F32),
            *rs, *rs, *sems,
        ],
        compiler_params=pltpu.CompilerParams(
            collective_id=0, has_side_effects=True, vmem_limit_bytes=60 * 2**20
        ),
        name="fused",
    )(
        queries, keys, values, key_bias.T, out_weight, moe_input, moe_gain.reshape(1, -1), route_ids.T, route_scores.T,
        shared_gate, shared_up, shared_down,
        expert_gate.reshape(2048, H), expert_up.reshape(2048, H), expert_down.reshape(H, 2048),
    )


def solution(mesh):
    return jax.shard_map(
        body,
        mesh=mesh,
        in_specs=(
            P("ep", "tp"), P("ep", "tp"), P("ep", "tp"), P("ep", "tp"), P("tp", None), P("ep", None), P(),
            P("ep", None), P("ep", None), P(None, "tp"), P(None, "tp"), P("tp", None),
            P("ep", None, "tp"), P("ep", None, "tp"), P("ep", "tp", None),
        ),
        out_specs=(P("ep", "tp"), P("ep", "tp")),
        check_vma=False,
    )
```

```python
import functools

import jax
import jax.numpy as jnp
from jax import lax
from jax.experimental import pallas as pl
from jax.experimental.pallas import tpu as pltpu
from jax.sharding import PartitionSpec as P

MESH = pl.DeviceIdType.MESH
BF = jnp.bfloat16
F32 = jnp.float32
NX, NZ, NY = 4, 8, 8
UP = 4
HELP = 3
SHIFT = UP + 1
BAND = 16
LOG2E = 1.4426950408889634
EPS_NORM = 1e-06
ROUTED_SCALE = 2.5
S = 512
H = 128
KB = 528
KVR = 1040
CAPP = 16
CAP = 12


def dot(a, b):
    return jnp.dot(a, b, preferred_element_type=F32)


def iota(shape, dim):
    return lax.broadcasted_iota(jnp.int32, shape, dim)


def attend(query, key, value, bias, first):
    half = S // 2
    logit = lax.dot_general(query, key, (((1,), (1,)), ((), ())), preferred_element_type=F32)
    logit = logit * (LOG2E / H**0.5) + bias
    soft = jnp.maximum(logit, jnp.log2(1.0 + jnp.exp2(jnp.minimum(logit, 100.0))))
    base = logit - soft
    if first is not None:
        visible = iota(soft.shape, 1) + first < iota(soft.shape, 0)
        soft = jnp.where(visible, soft, 0.0)
    soft = soft.astype(BF)
    later = jnp.where(iota((half, half), 0) > iota((half, half), 1), 1.0, 0.0).astype(BF)
    stay_hi = dot(soft[:, half:], later)
    sum_hi = stay_hi[:, 0:1] + soft[:, half : half + 1].astype(F32)
    stay_lo = dot(soft[:, :half], later) + sum_hi
    total = stay_lo[:, 0:1] + soft[:, 0:1].astype(F32)
    weight = jnp.exp2(base - jnp.concatenate([stay_lo, stay_hi], axis=1))
    if first is not None:
        weight = jnp.where(visible, weight, 0.0)
    return dot(weight.astype(BF), value), total


def kernel(
    q_in, k_in, v_in, bias_in, ow_in, mi_in, gain_in, ids_in, scores_in, sg_in, su_in, sd_in, eg_in, eu_in, ed_in,
    mixed, mix,
    qb, kvb, op, tcol, tr, ts, tr2, ts2, osend, orecv, hsend, hrecv, oacc, factor, heads,
    bias, gain, ids, scores, wgu, sgu, ed, sd, ow, mi, normed, gated,
    a1s, a1r, a2r, ag, b0, b1r, b2r, common,
    part_m, sib_m, ring_m, rsend_m, part_a, sib_a, ring_a, rsend_a,
    lsem, q_s, q_r, qh_s, qh_r, h_s, h_r, kv_s, kv_r, a1_s, a1_rs, a2_s, a2_rs, ag_s, ag_r, ags_s, ags_r,
    b1_s, b1_rs, b2_s, b2_rs, t_s, t_r, t2_s, t2_r, o_s, o_r,
    msib_s, msib_r, mring_s, mring_r, asib_s, asib_r, aring_s, aring_r,
):
    ep, tp = lax.axis_index("ep"), lax.axis_index("tp")
    z, x, y, c = ep // NX, ep % NX, tp // 2, tp % 2

    def at_x(d):
        return {"ep": z * NX + (x + d) % NX, "tp": tp}

    def at_z(d):
        return {"ep": ((z + d) % NZ) * NX + x, "tp": tp}

    def at_y(d):
        return {"ep": ep, "tp": ((y + d) % NY) * 2 + c}

    opposite = {"ep": (NZ - 1 - z) * NX + x, "tp": tp}

    helper, helped = z < HELP, z >= NZ - HELP
    sibling = {"ep": ep, "tp": y * 2 + (1 - c)}

    def send(src, dst, ssem, rsem, dev):
        return pltpu.make_async_remote_copy(
            src_ref=src, dst_ref=dst, send_sem=ssem, recv_sem=rsem, device_id=dev, device_id_type=MESH
        )

    local = [
        (q_in, qb.at[0, pl.ds(pl.multiple_of(x * S, S), S)]),
        (k_in, kvb.at[z, 0:S]),
        (v_in, kvb.at[z, KB:KVR]),
        (bias_in, bias),
        (mi_in, mi),
        (eg_in, wgu.at[:, 0:H]),
        (eu_in, wgu.at[:, H : 2 * H]),
        (sg_in, sgu.at[:, 0:H]),
        (su_in, sgu.at[:, H : 2 * H]),
        (ed_in, ed),
        (sd_in, sd),
        (ow_in, ow),
        (gain_in, gain),
        (ids_in, ids),
        (scores_in, scores),
    ]
    fetch = [pltpu.make_async_copy(a, b, lsem.at[i]) for i, (a, b) in enumerate(local)]

    barrier = pltpu.get_barrier_semaphore()
    partners = [at_x(d) for d in range(1, NX)] + [at_z(d) for d in range(1, NZ)]
    partners += [at_y(1), at_y(-1), sibling]
    for dev in partners:
        pl.semaphore_signal(barrier, inc=1, device_id=dev, device_id_type=MESH)
    for i in (4, 12, 13, 14, 3, 0, 1, 2, 5, 6, 7, 8, 9, 10, 11):
        fetch[i].start()

    pending = []

    def begin(copy, when=None):
        pending.append((when, copy))
        if when is None:
            copy.start()
        else:
            pl.when(when)(copy.start)

    halves = (slice(0, KB), slice(KB, KVR))

    def query_rows(i, which=0):
        return qb.at[which, pl.ds(pl.multiple_of(i * S, S), S)]

    def to_helper():
        return send(query_rows(x), query_rows(x, 1), qh_s.at[0], qh_r.at[0], opposite)

    def up(d, h):
        block = kvb.at[jnp.maximum(z - d + 1, 0), halves[h]]
        return send(block, block, kv_s.at[0, d - 1, h], kv_r.at[0, d - 1, h], at_z(1))

    def up_arrival(d, h):
        block = kvb.at[jnp.maximum(z - d, 0), halves[h]]
        return send(block, block, kv_s.at[0, d - 1, h], kv_r.at[0, d - 1, h], at_z(1))

    def down(d, h):
        block = kvb.at[jnp.minimum(z + d - 1, NZ - 1), halves[h]]
        return send(block, block, kv_s.at[1, d - 1, h], kv_r.at[1, d - 1, h], at_z(-1))

    def down_arrival(d, h):
        block = kvb.at[jnp.minimum(z + d, NZ - 1), halves[h]]
        return send(block, block, kv_s.at[1, d - 1, h], kv_r.at[1, d - 1, h], at_z(-1))

    def step(which, zi, place, first):
        rows = kvb[zi, S:KB, :].astype(F32) * LOG2E
        row = jnp.concatenate([rows[j : j + 1, :] for j in range(S // H)], axis=1)
        out, total = attend(qb[which], kvb[zi, 0:S, :], kvb[zi, KB:KVR, :], row, first)
        op[place] = out
        tcol[...] = jnp.where(iota((NX * S, H), 1) == place, total, tcol[...])

    def attention():
        fetch[0].wait()
        for d in range(1, NX):
            begin(send(query_rows(x), query_rows(x), q_s.at[d - 1], q_r.at[d - 1], at_x(d)))
        fetch[1].wait()
        sends_down = (z >= 1) & (z < HELP)
        begin(up(1, 0), z < NZ - 1)
        begin(down(1, 0), sends_down)
        fetch[2].wait()
        begin(up(1, 1), z < NZ - 1)
        begin(down(1, 1), sends_down)
        begin(to_helper(), helped)
        yield
        tcol[...] = jnp.zeros_like(tcol)
        for d in range(1, NX):
            src = query_rows((x - d + NX) % NX)
            send(src, src, q_s.at[d - 1], q_r.at[d - 1], at_x(d)).wait_recv()

        @pl.when(helper)
        def _():
            to_helper().wait_recv()

        for d in range(1, NX):
            begin(send(query_rows(x, 1), query_rows(x, 1), qh_s.at[d], qh_r.at[d], at_x(d)), helper)
        step(0, z, 0, x * S)
        yield
        def sums_of(qi):
            return tcol[qi * S : (qi + 1) * S].T[0:NZ, :]

        for d in range(1, UP + 1):
            for h in range(2):

                @pl.when(z >= d)
                def _():
                    up_arrival(d, h).wait_recv()

                if d < UP:
                    begin(up(d + 1, h), (z >= d) & (z < NZ - 1))
                if d == 1 or d == HELP:
                    hops = 1 if d == 1 else HELP - 1

                    @pl.when(z < HELP - hops)
                    def _():
                        down_arrival(hops, h).wait_recv()

                    if d == 1:
                        begin(down(2, h), z == 1)
            if d <= HELP:

                @pl.when(z == d - 1)
                def _():
                    for i in range(1, NX):
                        src = query_rows((x - i + NX) % NX, 1)
                        send(src, src, qh_s.at[i], qh_r.at[i], at_x(i)).wait_recv()

            mine = z >= d
            older = jnp.maximum(d - z - 1, 0)
            zi = jnp.where(mine, z - d, older)

            @pl.when(mine | (d <= HELP))
            def _():
                step(jnp.where(mine, 0, 1), zi, jnp.where(mine, d, SHIFT + older), None)

            if d == UP - 1:
                for qi in range(NX):
                    ts[qi] = sums_of(qi)
                for i in range(1, NX):
                    begin(send(ts, tr.at[x], t_s.at[i - 1], t_r.at[i - 1], at_x(i)))
                tr[x] = ts[...]
            yield
        newest = iota((NZ, S), 0) == UP
        for qi in range(NX):
            ts2[qi] = jnp.sum(jnp.where(newest, sums_of(qi), 0.0), axis=0, keepdims=True)
        for d in range(1, NX):
            begin(send(ts2, tr2.at[x], t2_s.at[d - 1], t2_r.at[d - 1], at_x(d)))
        tr2[x] = ts2[...]
        yield
        for d in range(1, NX):
            src, src2 = tr.at[(x - d + NX) % NX], tr2.at[(x - d + NX) % NX]
            send(ts, src, t_s.at[d - 1], t_r.at[d - 1], at_x(d)).wait_recv()
            send(ts2, src2, t2_s.at[d - 1], t2_r.at[d - 1], at_x(d)).wait_recv()

        def scales(qi):
            sums = [tr[i, qi] + jnp.where(newest, tr2[i, qi], 0.0) for i in range(NX)]
            row = sums[0] + sums[1] + sums[2] + sums[3]
            within = sum(jnp.where(i > x, sums[i], 0.0) for i in range(1, NX))
            parts, nothing = [None] * NZ, jnp.zeros((1, S), F32)
            run = nothing
            for k in range(SHIFT):
                parts[k] = run
                run = run + row[k : k + 1, :]
            after = nothing
            for k in reversed(range(SHIFT, NZ)):
                parts[k] = after
                after = after + row[k : k + 1, :]
            carried = jnp.concatenate(parts, axis=0) + within
            return [jnp.exp2(-carried), jnp.exp2(-run), jnp.zeros((BAND - NZ - 1, S), F32)]

        order = (1, 2, 3, 0)
        bands = [part for d in order for part in scales((x + d) % NX)]
        bands.append(jnp.zeros((H - NX * BAND, S), F32))
        scale = jnp.concatenate(bands, axis=0).T

        def share(j, k, rows):
            return scale[:, j * BAND + k : j * BAND + k + 1] * op[k, rows, :]

        def combine(j, rows):
            @pl.when(z >= UP)
            def _():
                total = share(j, 0, rows)
                for k in range(1, UP + 1):
                    total = total + share(j, k, rows)
                oacc[...] = total

            @pl.when(z < UP)
            def _():
                oacc[...] = share(j, 0, rows)
                for k in range(1, UP):

                    @pl.when(k <= z)
                    def _():
                        oacc[...] += share(j, k, rows)

        def combine_helped(j, d, rows):
            @pl.when(helper)
            def _():
                oacc[...] = share(j, SHIFT, rows)
                for i in range(1, HELP):

                    @pl.when(i < HELP - z)
                    def _():
                        oacc[...] += share(j, SHIFT + i, rows)

                if d > 0:
                    hsend[d - 1] = oacc[...].astype(BF)
                else:
                    factor[...] = oacc[...]

            if d > 0:
                begin(help_out(d), helper)

        def help_out(d):
            return send(hsend.at[d - 1], hrecv.at[d - 1], h_s.at[d], h_r.at[d], at_x(d))

        def help_home():
            return send(hsend.at[NX - 1], hrecv.at[NX - 1], h_s.at[0], h_r.at[0], opposite)

        for j, d in enumerate(order):
            combine_helped(j, d, pl.ds(pl.multiple_of(((x + d) % NX) * S, S), S))
        for j, d in enumerate(order):
            combine(j, pl.ds(pl.multiple_of(((x + d) % NX) * S, S), S))
            if d > 0:
                osend[d - 1] = oacc[...].astype(BF)
                begin(send(osend.at[d - 1], orecv.at[d - 1], o_s.at[d - 1], o_r.at[d - 1], at_x(d)))
            else:
                heads[...] = oacc[...]

                @pl.when(helped)
                def _():
                    factor[...] = jnp.broadcast_to(scale[:, j * BAND + NZ : j * BAND + NZ + 1], (S, H))

        yield

        @pl.when(helper)
        def _():
            for d in range(1, NX):
                help_out(d).wait_recv()
            far = factor[...] + hrecv[0].astype(F32) + hrecv[1].astype(F32) + hrecv[2].astype(F32)
            hsend[NX - 1] = far.astype(BF)

        begin(help_home(), helper)
        yield
        for d in range(1, NX):
            send(osend.at[d - 1], orecv.at[d - 1], o_s.at[d - 1], o_r.at[d - 1], at_x(d)).wait_recv()
        heads[...] += orecv[0].astype(F32) + orecv[1].astype(F32) + orecv[2].astype(F32)

        @pl.when(helped)
        def _():
            help_home().wait_recv()
            heads[...] += factor[...] * hrecv[NX - 1].astype(F32)

        rounded = heads[...].astype(BF)
        fetch[11].wait()

        def fill(yi):
            both = dot(rounded, ow[:, pl.ds(pl.multiple_of(yi * 256, 256), 256)]).astype(BF)
            part_a[0, yi] = both[:, :H]
            part_a[1, yi] = both[:, H:]

        out = yield from reduce_scatter(
            fill, 4, part_a, sib_a, ring_a, rsend_a, asib_s, asib_r, aring_s, aring_r
        )
        mixed[...] = out.astype(BF)

    def reduce_scatter(fill, cuts, part, sib, ring, rsend, sib_s, sib_r, ring_s, ring_r):
        order = [4, -3, 3, -2, 2, -1, 1, 0]
        length = S // cuts
        spans = [slice(i * length, (i + 1) * length) for i in range(cuts)]

        def to_sibling(m):
            yi = (y + order[m] + NY) % NY
            return send(part.at[1 - c, yi], sib.at[m], sib_s.at[m], sib_r.at[m], sibling)

        for m in range(NY):
            fill((y + order[m] + NY) % NY)
            begin(to_sibling(m))
        yield

        def mine(m, span):
            yi = (y + order[m] + NY) % NY
            return part[c, yi, span].astype(F32) + sib[m, span].astype(F32)

        def hop(way, s, i):
            return send(
                rsend.at[way, s, spans[i]], ring.at[way, s, spans[i]],
                ring_s.at[way, s, i], ring_r.at[way, s, i], at_y(1 - 2 * way),
            )

        for s in range(4):
            for i in range(cuts):
                for way in range(2):
                    if way == 1 and s == 3:
                        continue
                    if i == 0:
                        to_sibling(2 * s + way).wait_recv()
                    value = mine(2 * s + way, spans[i])
                    if s > 0:
                        hop(way, s - 1, i).wait_recv()
                        value = value + ring[way, s - 1, spans[i]].astype(F32)
                    rsend[way, s, spans[i]] = value.astype(BF)
                    begin(hop(way, s, i))
            yield
        to_sibling(7).wait_recv()
        done = []
        for i in range(cuts):
            value = mine(7, spans[i])
            hop(1, 2, i).wait_recv()
            value = value + ring[1, 2, spans[i]].astype(F32)
            hop(0, 3, i).wait_recv()
            done.append(value + ring[0, 3, spans[i]].astype(F32))
        return jnp.concatenate(done, axis=0) if cuts > 1 else done[0]

    def spread(transposed):
        shape = (NZ * NX * CAPP, NZ * NX * CAP) if transposed else (NZ * NX * CAP, NZ * NX * CAPP)
        padded, packed = (iota(shape, 0), iota(shape, 1)) if transposed else (iota(shape, 1), iota(shape, 0))
        place = padded & (CAPP - 1)
        hit = ((padded >> 4) * CAP + place == packed) & (place < CAP)
        return jnp.where(hit, 1.0, 0.0).astype(BF)

    def experts():
        for i in (4, 12, 13, 14):
            fetch[i].wait()
        value = mi[...].astype(F32)
        mean = jnp.mean(value * value, axis=1, keepdims=True)
        normed[...] = (value * lax.rsqrt(mean + EPS_NORM) * gain[...]).astype(BF)
        facing = ((y + NY // 2) % NY) * 2 + c
        own = jnp.concatenate([normed[:, pl.ds(pl.multiple_of(i * H, H), H)] for i in (tp, facing)], axis=1)
        slots = NZ * NX * CAPP
        group = iota((slots, 128), 0) >> 4
        place = iota((slots, 128), 0) & (CAPP - 1)
        expert = (group & (NZ - 1)) * NX + (group >> 3)
        first, second = ids[0:1, :] == expert, ids[1:2, :] == expert
        named = first | second
        earlier = jnp.where(iota((128, 128), 0) < iota((128, 128), 1), 1.0, 0.0).astype(BF)
        count = dot(jnp.where(named, 1.0, 0.0).astype(BF), earlier)
        chosen = named & (count == place.astype(F32))
        scale = ROUTED_SCALE / (scores[0:1, :] + scores[1:2, :])
        gate = jnp.where(first, scores[0:1, :] * scale, 0.0) + jnp.where(second, scores[1:2, :] * scale, 0.0)
        gated[...] = jnp.where(chosen, gate, 0.0)
        out = dot(jnp.where(chosen, 1.0, 0.0).astype(BF), own).astype(BF)
        a1s[...] = out.reshape(NX, NZ, CAPP, 2 * H)
        fetch[3].wait()
        line = bias[...]
        line = [line[:, j * H : (j + 1) * H] for j in range(S // H)]
        kvb[z, S:KB, :] = jnp.concatenate(line + [jnp.zeros((KB - S - S // H, H), BF)], axis=0)
        pl.semaphore_wait(barrier, len(partners))

        def by_x(d):
            return send(a1s.at[(x + d) % NX], a1r.at[x], a1_s.at[d - 1], a1_rs.at[d - 1], at_x(d))

        for d in range(1, NX):
            begin(by_x(d))
        a1r[x] = a1s[x]
        yield
        for d in range(1, NX):
            send(a1s.at[x], a1r.at[(x - d + NX) % NX], a1_s.at[d - 1], a1_rs.at[d - 1], at_x(d)).wait_recv()
        for d in range(1, NZ):
            begin(send(a1r.at[:, (z + d) % NZ], a2r.at[z], a2_s.at[d - 1], a2_rs.at[d - 1], at_z(d)))
        a2r[z] = a1r[:, z]
        yield
        for d in range(1, NZ):
            send(a1r.at[:, z], a2r.at[(z - d + NZ) % NZ], a2_s.at[d - 1], a2_rs.at[d - 1], at_z(d)).wait_recv()
        packed = dot(spread(False), a2r[...].reshape(slots, 2 * H)).astype(BF)
        ag[tp] = packed[:, :H]
        ag[facing] = packed[:, H:]

        def slice_of(yi, core=c):
            return ag.at[((yi + NY) % NY) * 2 + core]

        def along(way, n, yi):
            return send(slice_of(yi), slice_of(yi), ag_s.at[way, n], ag_r.at[way, n], at_y(1 - 2 * way))

        def across(m, yi, core):
            return send(slice_of(yi, core), slice_of(yi, core), ags_s.at[m], ags_r.at[m], sibling)

        for n in range(2):
            for way in range(2):
                begin(along(way, n, y + n * NY // 2))
        begin(across(0, y, c))
        begin(across(1, y + NY // 2, c))
        yield
        for way in range(2):
            near = y - (1 - 2 * way)
            along(way, 0, near).wait_recv()
            begin(along(way, 2, near))
            begin(across(2 + way, near, c))
        yield
        for n in range(1, 3):
            for way in range(2):
                sign = 1 - 2 * way
                came = y - sign + NY // 2 if n == 1 else y - 2 * sign
                along(way, n, came).wait_recv()
                begin(across(2 + 2 * n + way, came, c))
        yield
        across(0, y, 1 - c).wait_recv()
        across(1, y + NY // 2, 1 - c).wait_recv()
        for way in range(2):
            sign = 1 - 2 * way
            across(2 + way, y - sign, 1 - c).wait_recv()
            across(4 + way, y - sign + NY // 2, 1 - c).wait_recv()
            across(6 + way, y - 2 * sign, 1 - c).wait_recv()
        for i in (5, 6, 7, 8, 9, 10):
            fetch[i].wait()
        acc = jnp.zeros((NZ * NX * CAP, 2 * H), F32)
        acc_s = jnp.zeros((128, 2 * H), F32)
        for j in range(NY):
            wide = jnp.concatenate([ag[2 * j], ag[2 * j + 1]], axis=1)
            acc = acc + dot(wide, wgu[j * 256 : (j + 1) * 256, :])
            acc_s = acc_s + dot(normed[:, j * 256 : (j + 1) * 256], sgu[j * 256 : (j + 1) * 256, :])

        def swiglu(a):
            g, u = a[:, :H], a[:, H:]
            return (g / (1.0 + jnp.exp(-g)) * u).astype(BF)

        hidden, hidden_s = swiglu(acc), swiglu(acc_s)
        rows = NZ * NX * CAP

        def fill(yi):
            cols = pl.ds(pl.multiple_of(yi * 256, 256), 256)
            both = dot(hidden, ed[:, cols]).astype(BF)
            part_m[0, yi, 0:rows] = both[:, :H]
            part_m[1, yi, 0:rows] = both[:, H:]
            both = dot(hidden_s, sd[:, cols]).astype(BF)
            part_m[0, yi, rows:S] = both[:, :H]
            part_m[1, yi, rows:S] = both[:, H:]

        out = yield from reduce_scatter(
            fill, 2, part_m, sib_m, ring_m, rsend_m, msib_s, msib_r, mring_s, mring_r
        )
        common[...] = out[rows:S, :]
        b0[...] = dot(spread(True), out[0:rows, :].astype(BF)).astype(BF).reshape(NZ, NX, CAPP, H)
        for d in range(1, NZ):
            begin(send(b0.at[(z + d) % NZ], b1r.at[z], b1_s.at[d - 1], b1_rs.at[d - 1], at_z(d)))
        b1r[z] = b0[z]
        yield
        for d in range(1, NZ):
            send(b0.at[z], b1r.at[(z - d + NZ) % NZ], b1_s.at[d - 1], b1_rs.at[d - 1], at_z(d)).wait_recv()
        for d in range(1, NX):
            begin(send(b1r.at[:, (x + d) % NX], b2r.at[x], b2_s.at[d - 1], b2_rs.at[d - 1], at_x(d)))
        b2r[x] = b1r[:, x]
        yield
        for d in range(1, NX):
            send(b1r.at[:, x], b2r.at[(x - d + NX) % NX], b2_s.at[d - 1], b2_rs.at[d - 1], at_x(d)).wait_recv()
        gates = gated[...].T
        high = gates.astype(BF)
        low = (gates - high.astype(F32)).astype(BF)
        got = b2r[...].reshape(slots, H)
        mix[...] = (common[...] + dot(high, got) + dot(low, got)).astype(BF)

    attn, moe = attention(), experts()
    for turn in "mamamaamammamamamamaamaamama":
        next(attn if turn == "a" else moe, None)

    for when, copy in pending:
        if when is None:
            copy.wait_send()
        else:
            pl.when(when)(copy.wait_send)


def body(
    queries, keys, values, key_bias, out_weight, moe_input, moe_gain, route_ids, route_scores,
    shared_gate, shared_up, shared_down, expert_gate, expert_up, expert_down,
):
    hbm, vmem = pl.BlockSpec(memory_space=pl.ANY), pl.BlockSpec(memory_space=pltpu.VMEM)
    dma = pltpu.SemaphoreType.DMA
    V = pltpu.VMEM
    slots = (NZ, NX, CAPP, H)
    rs = [V((2, NY, S, H), BF), V((NY, S, H), BF), V((2, 4, S, H), BF), V((2, 4, S, H), BF)]
    sems = [dma((15,)), dma((3,)), dma((3,)), dma((4,)), dma((4,)), dma((4,)), dma((4,)), dma((2, 4, 2)), dma((2, 4, 2)), dma((3,)), dma((3,)), dma((7,)), dma((7,))]
    sems += [dma((2, 4)), dma((2, 4)), dma((8,)), dma((8,))]
    sems += [dma((7,)), dma((7,)), dma((3,)), dma((3,)), dma((3,)), dma((3,)), dma((3,)), dma((3,)), dma((3,)), dma((3,))]
    sems += [dma((8,)), dma((8,)), dma((2, 4, 4)), dma((2, 4, 4))] * 2
    return pl.pallas_call(
        kernel,
        out_shape=(jax.ShapeDtypeStruct((S, H), BF), jax.ShapeDtypeStruct((128, H), BF)),
        in_specs=[hbm] * 15,
        out_specs=(vmem, vmem),
        scratch_shapes=[
            V((2, NX * S, H), BF), V((NZ, KVR, H), BF), V((NZ, NX * S, H), F32), V((NX * S, H), F32),
            V((NX, NX, NZ, S), F32), V((NX, NZ, S), F32), V((NX, NX, 1, S), F32), V((NX, 1, S), F32),
            V((NX - 1, S, H), BF), V((NX - 1, S, H), BF),
            V((NX, S, H), BF), V((NX, S, H), BF), V((S, H), F32), V((S, H), F32), V((S, H), F32),
            V((1, S), BF), V((1, 2048), F32), V((2, 128), jnp.int32), V((2, 128), F32),
            V((2048, 2 * H), BF), V((2048, 2 * H), BF), V((H, 2048), BF), V((H, 2048), BF), V((H, 2048), BF),
            V((128, 2048), BF), V((128, 2048), BF), V((512, 128), F32),
            V((NX, NZ, CAPP, 2 * H), BF), V((NX, NZ, CAPP, 2 * H), BF), V((NZ, NX, CAPP, 2 * H), BF), V((16, NZ * NX * CAP, H), BF),
            V(slots, BF), V(slots, BF), V((NX, NZ, CAPP, H), BF), V((128, H), F32),
            *rs, *rs, *sems,
        ],
        compiler_params=pltpu.CompilerParams(
            collective_id=0, has_side_effects=True, vmem_limit_bytes=60 * 2**20
        ),
        name="fused",
    )(
        queries, keys, values, key_bias.T, out_weight, moe_input, moe_gain.reshape(1, -1), route_ids.T, route_scores.T,
        shared_gate, shared_up, shared_down,
        expert_gate.reshape(2048, H), expert_up.reshape(2048, H), expert_down.reshape(H, 2048),
    )


def solution(mesh):
    return jax.shard_map(
        body,
        mesh=mesh,
        in_specs=(
            P("ep", "tp"), P("ep", "tp"), P("ep", "tp"), P("ep", "tp"), P("tp", None), P("ep", None), P(),
            P("ep", None), P("ep", None), P(None, "tp"), P(None, "tp"), P("tp", None),
            P("ep", None, "tp"), P("ep", None, "tp"), P("ep", "tp", None),
        ),
        out_specs=(P("ep", "tp"), P("ep", "tp")),
        check_vma=False,
    )
```
